32 devices in a mesh: ep: 8 (over z, x), tp: 4 (over y, core).
Axes of the slice: x: 2, y: 2, z: 4, core: 2. Of those that a mesh axis runs over, the one named last changes fastest.
Arguments:
- tokens_first: bfloat16 [4096, 2048], P('ep'), may hold values from -6 to 6
- attn_gain: float32 [2048], replicated, may hold values from 0.1 to 1.9
- w_query: bfloat16 [2048, 1024], P(None, 'tp'), may hold values from -6 to 6
- key_matrix: bfloat16 [2048, 512], P(None, 'tp'), may hold values from -6 to 6
- value_matrix: bfloat16 [2048, 512], P(None, 'tp'), may hold values from -0.125 to 0.125
- head_sink_logit: float32 [16], P('tp'), may hold values from 1 to 5
- w_output: bfloat16 [1024, 2048], P('tp'), may hold values from -0.75 to 0.75
- tokens_second: bfloat16 [1024, 2048], P('ep'), may hold values from -6 to 6
- ffn_gain: float32 [2048], replicated, may hold values from 0.1 to 1.9
- routes: int32 [1024, 4], P('ep'), may hold values from 0 to 15, all different within a row; in each aligned block of 128 rows (0 to 127, 128 to 255, ...) at most 64 rows name the same one
- route_weight: float32 [1024, 4], P('ep'), may hold values from 0.2 to 1.5
- w_gate_exp: bfloat16 [16, 2048, 2048], P('ep', None, 'tp'), may hold values from -0.125 to 0.125
- w_up_exp: bfloat16 [16, 2048, 2048], P('ep', None, 'tp'), may hold values from -0.125 to 0.125
- w_down_exp: bfloat16 [16, 2048, 2048], P('ep', 'tp'), may hold values from -0.125 to 0.125
- w_gate_shared: bfloat16 [2048, 1024], P(None, 'tp'), may hold values from -0.125 to 0.125
- w_up_shared: bfloat16 [2048, 1024], P(None, 'tp'), may hold values from -0.125 to 0.125
- w_down_shared: bfloat16 [1024, 2048], P('tp'), may hold values from -0.1875 to 0.1875
Outputs:
- mixer_out: bfloat16 [4096, 2048], P(('ep', 'tp'))
- moe_out: bfloat16 [1024, 2048], P('ep', 'tp')
The draws below stay inside these ranges and needn't reach their ends.
Inputs may be any that keep to these rules, and one draw needn't show every extreme that they name: `routes`: each row names 4 different experts; among the rows of one index of ep no expert is named more than 64 times, a bound that some block reaches.
All inputs are finite; a program needn't handle non-finite values.
Results may differ from the reference program's by a relative error of at most 0.017.
Values may be sent and summed in bfloat16 or wider, within the bound.
A program may use at most 64 MiB of HBM per device.

```python
import math
import jax
import jax.numpy as jnp
import numpy as np
from jax import lax

MODEL_WIDTH = 2048
HEAD_SIZE = 64
QUERY_HEADS = 16
KEY_VALUE_HEADS = 8
BAND_LENGTH = 128
EFF = 2048
SFF = 1024
TOPK = 4
TOK1_DEV = 512
TOK2_DEV = 128
EXPERTS = 16
CAP = 64
TOKENS1 = 4096
TOKENS2 = 1024
N_EP = 8
N_TP = 4


def key_lookup(key):
    rotary_base = jax.random.normal(jax.random.fold_in(key, 7), (MODEL_WIDTH, KEY_VALUE_HEADS * HEAD_SIZE), jnp.float32)
    return jnp.clip(rotary_base, -6.0, 6.0) / math.sqrt(MODEL_WIDTH)


def draw_key_matrix(key, part):
    return key_lookup(key).astype(jnp.bfloat16)


def draw_w_query(key, part):
    rotary_base = jnp.clip(jax.random.normal(jax.random.fold_in(key, 11), (MODEL_WIDTH, QUERY_HEADS * HEAD_SIZE), jnp.float32), -6.0, 6.0) / math.sqrt(MODEL_WIDTH)
    return jnp.clip(rotary_base, -6.0, 6.0).astype(jnp.bfloat16)


def shard_levels(stream_key, dims, pieces, smallest, high):
    loudness = 1.0
    for position, shards_of in pieces:
        heights = jax.random.uniform(jax.random.fold_in(jax.random.fold_in(stream_key, 6), position), (shards_of,), jnp.float32, smallest / len(pieces), high / len(pieces))
        loudness = loudness * jnp.repeat(jnp.exp(heights), dims[position] // shards_of).reshape((-1,) + (1,) * (len(dims) - 1 - position))
    return loudness


def assign_block(key, own, number, rows, number_of, top, most, lean):
    ranking = jax.random.permutation(key, number_of)
    crowded, ordinary = portions_of(number_of, rows * top, most, lean, True), portions_of(number_of, rows * top, most, lean, False)
    places = jnp.arange(number_of)

    def named(tallies, offset_by):
        used = int((tallies > 0).sum())
        fixed = max(1, used // 4)
        shifted = fixed + (places - fixed + offset_by * (used - fixed)) % max(1, number_of - fixed)
        return jnp.zeros((number_of,), jnp.int32).at[ranking[jnp.where(places < fixed, places, shifted)]].set(jnp.asarray(tallies, jnp.int32))

    tallies = jnp.where(number % 4 == 0, named(crowded, number // 4), named(ordinary, number - number // 4 - 1))
    mixed = jax.random.permutation(jax.random.fold_in(own, 3), number_of)
    source_of, receiver = mixed[0:number_of // 2 * 2:2], mixed[1:number_of // 2 * 2:2]
    margin = jnp.minimum(tallies[source_of] - 1, most - tallies[receiver]) // 2
    margin = jnp.where((source_of == ranking[0]) | (receiver == ranking[0]) | (tallies[receiver] == 0), 0, jnp.maximum(margin, 0))
    shifted = jax.random.randint(jax.random.fold_in(own, 4), (number_of // 2,), 0, 1 << 20) % (margin + 1)
    tallies = tallies.at[source_of].add(-shifted).at[receiver].add(shifted)
    labels = jnp.searchsorted(jnp.cumsum(tallies), jnp.arange(rows * top), side="right").astype(jnp.int32)
    listing = labels.reshape(top, rows).T
    listing = listing[jax.random.permutation(jax.random.fold_in(own, 1), rows)]
    offset_by = jax.random.randint(jax.random.fold_in(own, 2), (rows, 1), 0, top)
    return jnp.take_along_axis(listing, (jnp.arange(top)[None, :] + offset_by) % top, axis=1)


def portions_of(number_of, total, bound, lean, full):
    portions = [(1 << 20) // math.isqrt(rank ** lean) + 1 for rank in range(1, number_of + 1)]
    largest = bound if full else min(bound, max(-(-total // number_of), total * portions[0] // sum(portions)))
    least = 1 if total - largest >= number_of - 1 else 0
    given, surplus = [largest] + [least] * (number_of - 1), total - largest - least * (number_of - 1)
    while surplus > 0:
        free = [i for i in range(1, number_of) if given[i] < largest] or [i for i in range(1, number_of) if given[i] < bound]
        mass, left = sum([portions[i] for i in free]), surplus
        for i in free:
            extra = min(bound - given[i], max(1, left * portions[i] // mass), surplus)
            given[i] = given[i] + extra
            surplus = surplus - extra
    return np.array(given)


def scatter_about(key, extent, spread, bound, pieces=(), kind=jnp.bfloat16):
    level = shard_levels(key, extent, pieces, -0.22, 0.18) if pieces else 1.0
    values = jax.random.normal(key, extent, jnp.float32) * spread * level
    return jnp.minimum(jnp.maximum(values, -bound), bound).astype(kind)


def setup_inputs(seed: int = 0) -> dict:
    arg_keys = jax.random.split(jax.random.key(seed), 18)
    tokens_first = scatter_about(arg_keys[0], (TOKENS1, MODEL_WIDTH), 1.0, 6.0, ((0, 8),))
    attn_gain = jnp.clip(1.0 + 0.18 * jax.random.normal(arg_keys[1], (MODEL_WIDTH,), jnp.float32), 0.1, 1.9)
    w_query = draw_w_query(jax.random.fold_in(arg_keys[17], 71), 0)
    key_matrix = draw_key_matrix(jax.random.fold_in(arg_keys[17], 71), 0)
    value_matrix = scatter_about(arg_keys[4], (MODEL_WIDTH, KEY_VALUE_HEADS * HEAD_SIZE), MODEL_WIDTH ** -0.5, 0.125, ((1, 4),))
    head_sink_logit = jnp.clip(1.0 + 4.0 * jax.random.uniform(arg_keys[5], (QUERY_HEADS,), jnp.float32) ** shard_levels(arg_keys[5], (QUERY_HEADS,), ((0, 4),), -0.2, 0.2), 1.0, 5.0)
    w_output = scatter_about(arg_keys[6], (QUERY_HEADS * HEAD_SIZE, MODEL_WIDTH), (QUERY_HEADS * HEAD_SIZE // 16) ** -0.5, 0.75, ((0, 4),))
    tokens_second = scatter_about(arg_keys[7], (TOKENS2, MODEL_WIDTH), 1.0, 6.0, ((0, 8),))
    ffn_gain = jnp.clip(1.0 + 0.18 * jax.random.normal(arg_keys[8], (MODEL_WIDTH,), jnp.float32), 0.1, 1.9)
    routes_keys = jax.random.split(jax.random.fold_in(arg_keys[9], 1), TOKENS2 // TOK2_DEV)
    routes_turns = jax.random.permutation(jax.random.fold_in(arg_keys[9], 3), TOKENS2 // TOK2_DEV)
    routes = jax.vmap(lambda own, number: assign_block(jax.random.fold_in(arg_keys[9], 2), own, number, TOK2_DEV, EXPERTS, TOPK, CAP, 2))(routes_keys, routes_turns).reshape((TOKENS2, TOPK))
    route_weight = jnp.clip(0.2 + 1.3 * jax.random.uniform(arg_keys[10], (TOKENS2, TOPK), jnp.float32) ** shard_levels(arg_keys[10], (TOKENS2, TOPK), ((0, 8),), -0.2, 0.2), 0.2, 1.5)
    w_gate_exp = scatter_about(arg_keys[11], (EXPERTS, MODEL_WIDTH, EFF), MODEL_WIDTH ** -0.5, 0.125, ((0, 8), (2, 4)))
    w_up_exp = scatter_about(arg_keys[12], (EXPERTS, MODEL_WIDTH, EFF), MODEL_WIDTH ** -0.5, 0.125, ((0, 8), (2, 4)))
    w_down_exp = scatter_about(arg_keys[13], (EXPERTS, EFF, MODEL_WIDTH), EFF ** -0.5, 0.125, ((0, 8), (1, 4)))
    w_gate_shared = scatter_about(arg_keys[14], (MODEL_WIDTH, SFF), MODEL_WIDTH ** -0.5, 0.125, ((1, 4),))
    w_up_shared = scatter_about(arg_keys[15], (MODEL_WIDTH, SFF), MODEL_WIDTH ** -0.5, 0.125, ((1, 4),))
    w_down_shared = scatter_about(arg_keys[16], (SFF, MODEL_WIDTH), SFF ** -0.5, 0.1875, ((0, 4),))
    return dict(tokens_first=tokens_first, attn_gain=attn_gain, w_query=w_query, key_matrix=key_matrix, value_matrix=value_matrix, head_sink_logit=head_sink_logit, w_output=w_output, tokens_second=tokens_second, ffn_gain=ffn_gain, routes=routes, route_weight=route_weight, w_gate_exp=w_gate_exp, w_up_exp=w_up_exp, w_down_exp=w_down_exp, w_gate_shared=w_gate_shared, w_up_shared=w_up_shared, w_down_shared=w_down_shared)


rope_base = 10000.0
norm_eps = 1e-06

def rms_scale(inputs, gain):
    wide = inputs.astype(jnp.float32)
    scaled = wide * lax.rsqrt(lax.optimization_barrier(jnp.mean(wide * wide, axis=-1, keepdims=True)) + norm_eps)
    return (scaled * gain).astype(jnp.bfloat16)

def apply_rotary(heads, token_positions):
    freqs = rope_base ** (-jnp.arange(0, HEAD_SIZE, 2, dtype=jnp.float32) / HEAD_SIZE)
    angles = token_positions[:, None] * freqs[None, :]
    cosine = jnp.cos(angles)[:, None, :]
    sine = jnp.sin(angles)[:, None, :]
    first_half, second_half = jnp.split(heads, 2, axis=-1)
    return jnp.concatenate([first_half * cosine - second_half * sine, second_half * cosine + first_half * sine], axis=-1)

def group_sum(rows, weights, groups):
    width = rows.shape[1] // groups
    parts = jnp.einsum('rtc,tcd->trd', rows.reshape(rows.shape[0], groups, width).astype(jnp.float32), weights.reshape(groups, width, weights.shape[1]).astype(jnp.float32))
    return lax.optimization_barrier(jnp.sum(parts.astype(jnp.bfloat16).astype(jnp.float32), axis=0))

def reference(tokens_first, attn_gain, w_query, key_matrix, value_matrix, head_sink_logit, w_output, tokens_second, ffn_gain, routes, route_weight, w_gate_exp, w_up_exp, w_down_exp, w_gate_shared, w_up_shared, w_down_shared):
    first_count = tokens_first.shape[0]
    norm_input = rms_scale(tokens_first, attn_gain)
    token_positions = jnp.arange(first_count, dtype=jnp.int32).astype(jnp.float32)
    query_rows = apply_rotary(jnp.dot(norm_input, w_query, preferred_element_type=jnp.float32).reshape(first_count, QUERY_HEADS, HEAD_SIZE), token_positions).astype(jnp.bfloat16)
    key_rows = apply_rotary(jnp.dot(norm_input, key_matrix, preferred_element_type=jnp.float32).reshape(first_count, KEY_VALUE_HEADS, HEAD_SIZE), token_positions).astype(jnp.bfloat16)
    value_rows = jnp.dot(norm_input, value_matrix, preferred_element_type=jnp.float32).astype(jnp.bfloat16).reshape(first_count, KEY_VALUE_HEADS, HEAD_SIZE)
    pad_rows = jnp.zeros((BAND_LENGTH, KEY_VALUE_HEADS, HEAD_SIZE), jnp.bfloat16)
    keys_padded = jnp.concatenate([pad_rows, key_rows], axis=0)
    values_padded = jnp.concatenate([pad_rows, value_rows], axis=0)
    layer_block = min(512, TOK1_DEV)
    head_group = QUERY_HEADS // KEY_VALUE_HEADS
    sink_scores = head_sink_logit.astype(jnp.float32).reshape(KEY_VALUE_HEADS, head_group)[:, :, None, None]

    def attend(index):
        leading_row = index * layer_block
        block_queries = lax.dynamic_slice_in_dim(query_rows, leading_row, layer_block, 0).reshape(layer_block, KEY_VALUE_HEADS, head_group, HEAD_SIZE).astype(jnp.float32)
        key_block = lax.dynamic_slice_in_dim(keys_padded, leading_row, layer_block + BAND_LENGTH, 0).astype(jnp.float32)
        value_block = lax.dynamic_slice_in_dim(values_padded, leading_row, layer_block + BAND_LENGTH, 0).astype(jnp.float32)
        scores = jnp.einsum('qhgd,khd->hgqk', block_queries, key_block) * HEAD_SIZE ** (-0.5)
        query_pos = leading_row + jnp.arange(layer_block, dtype=jnp.int32)
        key_pos = leading_row - BAND_LENGTH + jnp.arange(layer_block + BAND_LENGTH, dtype=jnp.int32)
        offsets = query_pos[:, None] - key_pos[None, :]
        visible = (offsets >= 0) & (offsets < BAND_LENGTH) & (key_pos[None, :] >= 0)
        scores = jnp.where(visible[None, None], scores, -jnp.inf)
        peak = jnp.maximum(lax.optimization_barrier(jnp.max(scores, axis=-1, keepdims=True)), sink_scores)
        expo = jnp.exp(scores - peak)
        total = lax.optimization_barrier(jnp.sum(expo, axis=-1, keepdims=True)) + jnp.exp(sink_scores - peak)
        weights = (expo / total).astype(jnp.bfloat16)
        mixed = jnp.einsum('hgqk,khd->qhgd', weights.astype(jnp.float32), value_block)
        return mixed.astype(jnp.bfloat16).reshape(layer_block, QUERY_HEADS * HEAD_SIZE)
    attended = lax.map(attend, jnp.arange(first_count // layer_block, dtype=jnp.int32)).reshape(first_count, QUERY_HEADS * HEAD_SIZE)

    def project(rows):
        return group_sum(rows, w_output, N_TP).astype(jnp.bfloat16)
    mixer_out = lax.map(project, attended.reshape(N_EP, TOK1_DEV, QUERY_HEADS * HEAD_SIZE)).reshape(first_count, MODEL_WIDTH)
    count_second = tokens_second.shape[0]
    normed_second = rms_scale(tokens_second, ffn_gain)
    flat = routes.reshape(N_EP, TOK2_DEV * TOPK)
    onehot = (flat[:, :, None] == jnp.arange(EXPERTS, dtype=jnp.int32)[None, None, :]).astype(jnp.int32)
    ranks = lax.optimization_barrier(jnp.sum((jnp.cumsum(onehot, axis=1) - onehot) * onehot, axis=-1))
    sources = jnp.arange(N_EP, dtype=jnp.int32)[:, None]
    slots = (flat * (N_EP * CAP) + sources * CAP + ranks).reshape(count_second * TOPK).astype(jnp.int32)
    row_ids = jnp.repeat(jnp.arange(count_second, dtype=jnp.int32), TOPK)
    buffer = jnp.zeros((EXPERTS * N_EP * CAP, MODEL_WIDTH), jnp.bfloat16).at[slots].set(normed_second[row_ids])

    def expert(operands):
        rows, gate_w, up_w, down_w = operands
        gate_pre = jnp.dot(rows, gate_w, preferred_element_type=jnp.float32)
        up_pre = jnp.dot(rows, up_w, preferred_element_type=jnp.float32)
        hidden = (jax.nn.silu(gate_pre) * up_pre).astype(jnp.bfloat16)
        return group_sum(hidden, down_w, N_TP).astype(jnp.bfloat16)
    results = lax.map(expert, (buffer.reshape(EXPERTS, N_EP * CAP, MODEL_WIDTH), w_gate_exp, w_up_exp, w_down_exp)).reshape(-1, MODEL_WIDTH)
    chosen = results[slots].reshape(count_second, TOPK, MODEL_WIDTH).astype(jnp.float32)
    routed = lax.optimization_barrier(jnp.sum(chosen * route_weight.astype(jnp.float32)[:, :, None], axis=1))
    shared_hidden = (jax.nn.silu(jnp.dot(normed_second, w_gate_shared, preferred_element_type=jnp.float32)) * jnp.dot(normed_second, w_up_shared, preferred_element_type=jnp.float32)).astype(jnp.bfloat16)
    shared_sum = group_sum(shared_hidden, w_down_shared, N_TP)
    moe_out = (routed + shared_sum).astype(jnp.bfloat16)
    return (mixer_out, moe_out)
```

```python
import functools
import jax
import jax.numpy as jnp
import numpy as np
from jax import lax
from jax.experimental import pallas as pl
from jax.experimental.pallas import tpu as pltpu
from jax.sharding import PartitionSpec as P

MODEL_WIDTH = 2048
HEAD_SIZE = 64
BAND_LENGTH = 128


rope_base = 10000.0
norm_eps = 1e-06


def from_behind(value, axis, by):
    devices = lax.axis_size(axis)
    pairs = [(i, i + by) for i in range(devices) if 0 <= i + by < devices]
    return lax.ppermute(value, axis, pairs)


def rms_scale(inputs, gain):
    wide = inputs.astype(jnp.float32)
    scaled = wide * lax.rsqrt(jnp.mean(wide * wide, axis=-1, keepdims=True) + norm_eps)
    return (scaled * gain).astype(jnp.bfloat16)


def apply_rotary(heads, token_positions):
    freqs = rope_base ** (-jnp.arange(0, HEAD_SIZE, 2, dtype=jnp.float32) / HEAD_SIZE)
    angles = token_positions[:, None] * freqs[None, :]
    cosine = jnp.cos(angles)[:, None, :]
    sine = jnp.sin(angles)[:, None, :]
    first_half, second_half = jnp.split(heads, 2, axis=-1)
    return jnp.concatenate(
        [first_half * cosine - second_half * sine, second_half * cosine + first_half * sine],
        axis=-1,
    )


MESH = pl.DeviceIdType.MESH
F32 = jnp.float32
BF16 = jnp.bfloat16


def dot(a, b):
    return jnp.dot(a, b, preferred_element_type=F32)


def lanes_of(shape):
    return lax.broadcasted_iota(jnp.int32, shape, len(shape) - 1)


def fused_kernel(
    cap,
    sinks, ag_h, fg_h, rt_h, rw_h, fine_h, coarse_h, tf_h, wq_h, wk_h, wv_h, wo_h, ts_h,
    wg_h, wu_h, wd_h, sg_h, su_h, sd_h,
    mix_out, moe_out,
    ag, fg, rt, rw, fine, coarse, tf, wq, wk, wv, wo, ts, wg, wu, wd, sg, su, sd,
    qs, kd, vd, halo_s, halo_r, xg, mg, oh, oht, wsl, xs, hid, tokh, shh,
    mp, mrc, ms, mry, mo_own, mo_peer, rc, s1x, rx1, s1y, ry1, s2y, ry2, s2x, rx2, s3, rz, keep,
    lsem, ss, rs,
):
    me, t = lax.axis_index("ep"), lax.axis_index("tp")
    z, x, y, c = me // 2, me % 2, t // 2, t % 2
    zs = (z, z + 1 - 2 * (z % 2), (z + 2) % 4, 3 - z)
    z_peer = [{"ep": zd * 2 + x, "tp": t} for zd in zs]
    x_peer = {"ep": z * 2 + 1 - x, "tp": t}
    y_peer = {"ep": me, "tp": (1 - y) * 2 + c}
    c_peer = {"ep": me, "tp": y * 2 + 1 - c}
    n_ep = 8
    exp_dev = wg.shape[0]
    topk = rt.shape[0]
    rows = ts.shape[0]
    blocks = tf.shape[0] // rows

    loads = {}

    def load(name, src, dst):
        k = pltpu.make_async_copy(src, dst, lsem.at[len(loads)])
        k.start()
        loads[name] = k

    def need(*names):
        for name in names:
            k = loads.pop(name, None)
            if k is not None:
                done.append(name)
                k.wait()

    done = []
    pairs = [
        ("ts", ts_h, ts), ("fg", fg_h, fg), ("rt", rt_h, rt), ("rw", rw_h, rw), ("ag", ag_h, ag),
        ("tf", tf_h, tf), ("fine", fine_h, fine), ("coarse", coarse_h, coarse), ("wq", wq_h, wq),
        ("wk", wk_h, wk), ("wv", wv_h, wv), ("wo", wo_h, wo), ("sg", sg_h, sg), ("su", su_h, su),
        ("wg", wg_h, wg), ("wu", wu_h, wu), ("wd", wd_h, wd), ("sd", sd_h, sd),
    ]
    for name, a, b in pairs:
        load(name, a, b)

    barrier = pltpu.get_barrier_semaphore()
    for e in range(1, n_ep):
        pl.semaphore_signal(
            barrier, inc=1, device_id={"ep": (me + e) % n_ep, "tp": t}, device_id_type=MESH
        )
    for peer in (y_peer, c_peer):
        pl.semaphore_signal(barrier, inc=1, device_id=peer, device_id_type=MESH)

    ids = {}
    started = []

    def copy(name, src, dst, peer):
        i = ids.setdefault(name, len(ids))
        return pltpu.make_async_remote_copy(
            src_ref=src, dst_ref=dst, send_sem=ss.at[i], recv_sem=rs.at[i],
            device_id=peer, device_id_type=MESH,
        )

    def send(name, src, dst, peer):
        k = copy(name, src, dst, peer)
        k.start()
        started.append(k)

    def got(name, dst):
        copy(name, dst, dst, c_peer).wait_recv()

    def normed(wide, gain):
        return (
            wide * lax.rsqrt(jnp.mean(wide * wide, axis=-1, keepdims=True) + norm_eps) * gain
        ).astype(BF16)

    def R(d, s):
        return s * 4 + d

    own = R(0, 1)
    quarter = xg.shape[3]

    def q_of(k, cc):
        return (y if k else 1 - y) * 2 + cc

    need("ts", "fg", "rt", "rw")
    xn = normed(ts[...].astype(F32), fg[...])
    for q in range(4):
        xg[own, q] = xn[:, q * quarter : (q + 1) * quarter]
    mg[own] = jnp.concatenate([rt[...].astype(F32), rw[...]], axis=0)
    pl.semaphore_wait(barrier, n_ep + 1)

    def block_send(link, d, s, k, peer, at):
        send((link, at, k), xg.at[R(d, s), q_of(k, c)], xg.at[at, q_of(k, c)], peer)

    block_send("z", 0, 1, 1, z_peer[1], R(1, 1))
    block_send("x", 0, 1, 1, x_peer, R(0, 0))
    block_send("z", 0, 1, 1, z_peer[2], R(2, 1))
    block_send("z", 0, 1, 1, z_peer[3], R(3, 1))
    block_send("z", 0, 1, 0, z_peer[1], R(1, 1))
    block_send("x", 0, 1, 0, x_peer, R(0, 0))
    for s in (0, 1):
        for d in range(4):
            if R(d, s) != own:
                peer = {"ep": zs[d] * 2 + (x if s else 1 - x), "tp": t}
                send(("m", R(d, s)), mg.at[own], mg.at[R(d, s)], peer)

    c_list = {}

    def to_core(at, k):
        c_list[(at, k)] = True
        send(("c", at, k), xg.at[at, q_of(k, c)], xg.at[at, q_of(k, c)], c_peer)

    def to_x(d):
        send(("x", R(d, 0), 1), xg.at[R(d, 1), q_of(1, c)], xg.at[R(d, 0), q_of(1, c)], x_peer)

    def to_y(at):
        send(("y", at), xg.at[at, q_of(1, c)], xg.at[at, q_of(1, c)], y_peer)

    def arrived(link, at, k):
        got((link, at, k), xg.at[at, q_of(k, c)])

    def from_y(at):
        got(("y", at), xg.at[at, q_of(0, c)])
        to_core(at, 0)

    def from_core(at):
        for k in (1, 0):
            got(("c", at, k), xg.at[at, q_of(k, 1 - c)])

    lane = lanes_of((rows, 128))
    low = lane % 64 < 32
    left = lane < 64

    def qkv(b):
        part = slice(b * rows, (b + 1) * rows)
        nb = normed(tf[part].astype(F32), ag[...])
        base = pl.ds(me * blocks + b, 1)
        cb, sb = coarse[0, base, :], coarse[1, base, :]
        cosine = fine[0] * cb - fine[1] * sb
        sine = fine[1] * cb + fine[0] * sb
        sine = jnp.where(low, -sine, sine)

        def rot(v):
            swap = jnp.where(low, pltpu.roll(v, 96, 1), pltpu.roll(v, 32, 1))
            return v * cosine + swap * sine

        need("wk")
        kk = rot(dot(nb, wk[...]))
        need("wv")
        vv = dot(nb, wv[...])
        store_kv(kk.astype(BF16).astype(F32), vv.astype(BF16).astype(F32), (b + 1) * rows)
        if b == blocks - 1:
            halo_s[:, 0:128] = kk.astype(BF16)
            halo_s[:, 128:256] = vv.astype(BF16)
        need("wq")
        for g in range(2):
            qq = rot(dot(nb, wq[:, g * 128 : (g + 1) * 128])) * HEAD_SIZE ** (-0.5)
            qs[part, g * 128 : (g + 1) * 128] = qq.astype(BF16)

    def store_kv(kk, vv, at):
        for ref, val in ((kd, kk), (vd, vv)):
            other = pltpu.roll(val, 64, 1)
            ref[0, at : at + rows, :] = jnp.where(left, val, other).astype(BF16)
            ref[1, at : at + rows, :] = jnp.where(left, other, val).astype(BF16)

    i2 = lax.broadcasted_iota(jnp.int32, (2 * rows, 2 * rows), 0)
    band = lanes_of((2 * rows, 2 * rows)) - i2 % rows
    top = lax.broadcasted_iota(jnp.int32, (2 * rows, 1), 0) < rows

    def attend(b):
        part = slice(b * rows, (b + 1) * rows)
        outs = []
        visible = (band > 0) & (band <= rows)
        if b == 0:
            visible = visible & ((lanes_of((2 * rows, 2 * rows)) >= rows) | (me > 0))
        for g in range(2):
            q2 = qs[part, g * 128 : (g + 1) * 128]
            zero = jnp.zeros_like(q2)
            qq = jnp.concatenate([jnp.where(left, q2, zero), jnp.where(left, zero, q2)], axis=0)
            score = lax.dot_general(
                qq, kd[g, b * rows : (b + 2) * rows, :], (((1,), (1,)), ((), ())),
                preferred_element_type=F32,
            )
            score = jnp.where(visible, score, -jnp.inf)
            sink = jnp.where(top, sinks[2 * g], sinks[2 * g + 1])
            peak = jnp.maximum(jnp.max(score, axis=-1, keepdims=True), sink)
            expo = jnp.exp(score - peak)
            total = jnp.sum(expo, axis=-1, keepdims=True) + jnp.exp(sink - peak)
            weights = (expo * (1.0 / total)).astype(BF16)
            o = dot(weights, vd[g, b * rows : (b + 2) * rows, :])
            outs.append(jnp.where(left, o[:rows], o[rows:]).astype(BF16))
        att = jnp.concatenate(outs, axis=1)
        need("wo")
        for n in range(4):
            mp[b, :, n * 512 : (n + 1) * 512] = dot(att, wo[:, n * 512 : (n + 1) * 512]).astype(BF16)

    def onehots():
        for s in (0, 1):
            for d in range(4):
                if R(d, s) != own:
                    got(("m", R(d, s)), mg.at[R(d, s)])
        before = (
            lax.broadcasted_iota(jnp.int32, (rows, rows), 0)
            < lax.broadcasted_iota(jnp.int32, (rows, rows), 1)
        ).astype(F32).astype(BF16)
        hits, vals = [], []
        for r in range(n_ep):
            for e in range(exp_dev):
                named = mg[r, 0:topk, :] == (me * exp_dev + e).astype(F32)
                hits.append(jnp.sum(named.astype(F32), axis=0, keepdims=True))
                vals.append(
                    jnp.sum(jnp.where(named, mg[r, topk : 2 * topk, :], 0.0), axis=0, keepdims=True)
                )
        ranks = dot(jnp.concatenate(hits, axis=0).astype(BF16), before)
        slot = lax.broadcasted_iota(jnp.int32, (cap, rows), 0).astype(F32)
        for r in range(n_ep):
            both = []
            for e in range(exp_dev):
                i = r * exp_dev + e
                at = (slot == ranks[i : i + 1, :]) & (hits[i] > 0.0)
                both.append(at.astype(F32))
                wsl[r, e] = jnp.sum(jnp.where(at, vals[i], 0.0), axis=1, keepdims=True)
            full = jnp.concatenate(both, axis=0)
            oh[r] = full.astype(BF16)
            turned = full.T
            for e in range(exp_dev):
                oht[r, e] = jnp.where(lanes_of(turned.shape) // cap == e, turned, 0.0).astype(BF16)

    def shared_hidden():
        need("sg", "su")
        g = jnp.zeros((rows, sg.shape[1]), F32)
        u = jnp.zeros((rows, sg.shape[1]), F32)
        for q in range(4):
            part = slice(q * quarter, (q + 1) * quarter)
            g = g + dot(xg[own, q], sg[part, :])
            u = u + dot(xg[own, q], su[part, :])
        shh[...] = (g / (1.0 + jnp.exp(-g)) * u).astype(BF16)

    half = 4 * cap

    def dispatch(h, group):
        for i, r in enumerate(group):
            for q in range(4):
                v = dot(oh[r], xg[r, q]).astype(BF16)
                for e in range(exp_dev):
                    xs[e, h * half + i * cap : h * half + (i + 1) * cap,
                       q * quarter : (q + 1) * quarter] = v[e * cap : (e + 1) * cap]

    def gate_up(h, group, e):
        need("wg", "wu")
        rin = slice(h * half, (h + 1) * half)
        wcol = jnp.concatenate([wsl[r, e] for r in group], axis=0)
        for n in range(2):
            cs = slice(n * 256, (n + 1) * 256)
            g = dot(xs[e, rin, :], wg[e, :, cs])
            u = dot(xs[e, rin, :], wu[e, :, cs])
            hh = (g / (1.0 + jnp.exp(-g)) * u * wcol).astype(BF16)
            for i, r in enumerate(group):
                hid[r * rows + e * cap : r * rows + (e + 1) * cap, cs] = hh[i * cap : (i + 1) * cap]

    def to_tokens(group):
        width = hid.shape[1]
        for r in group:
            for e in range(exp_dev):
                tokh[r * rows : (r + 1) * rows, e * width : (e + 1) * width] = dot(
                    oht[r, e], hid[r * rows : (r + 1) * rows, :]
                ).astype(BF16)

    ysel = (1 - y, y)

    def down(jj, yr, dst, cc):
        need("wd", "sd")
        width = hid.shape[1]
        base = pl.multiple_of((ysel[yr] * 2 + cc) * 512 + jj * 256, 256)
        cs = pl.ds(base, 256)
        for rb in range(4):
            part = slice(rb * 256, (rb + 1) * 256)
            o = dot(tokh[part, 0:width], wd[0, :, cs]) + dot(tokh[part, width : 2 * width], wd[1, :, cs])
            if rb == own * rows // 256:
                extra = dot(shh[...], sd[:, cs])
                o = jnp.concatenate([o[:rows] + extra, o[rows:]], axis=0)
            dst[jj, yr, 0, part, :] = o[:, 0:128].astype(BF16)
            dst[jj, yr, 1, part, :] = o[:, 128:256].astype(BF16)

    def core_send(jj):
        for yr in range(2):
            for o in range(2):
                send(("rc", jj, yr, o), mo_peer.at[jj, yr, o], rc.at[jj, yr, o], c_peer)

    def both(jj, yr, o, part):
        return mo_own[jj, yr, o, part, :].astype(F32) + rc[jj, yr, o, part, :].astype(F32)

    far, near = slice(0, 512), slice(512, 1024)

    def stage1(jj):
        for yr in range(2):
            for o in range(2):
                got(("rc", jj, yr, o), rc.at[jj, yr, o])
        for yr in range(2):
            s1x[jj, yr] = both(jj, yr, 0, far).astype(BF16)
        send(("rx1", jj), s1x.at[jj], rx1.at[jj], x_peer)
        s1y[jj] = both(jj, 0, 1, slice(0, 1024)).astype(BF16)
        send(("ry1", jj), s1y.at[jj], ry1.at[jj], y_peer)

    def stage2(jj):
        got(("rx1", jj), rx1.at[jj])
        s2y[jj] = (both(jj, 0, 0, near) + rx1[jj, 0].astype(F32)).astype(BF16)
        send(("ry2", jj), s2y.at[jj], ry2.at[jj], y_peer)
        got(("ry1", jj), ry1.at[jj])
        s2x[jj] = (both(jj, 1, 1, far) + ry1[jj, far, :].astype(F32)).astype(BF16)
        send(("rx2", jj), s2x.at[jj], rx2.at[jj], x_peer)

    def stage3(jj, o):
        if o == 0:
            got(("ry2", jj), ry2.at[jj])
        else:
            got(("rx2", jj), rx2.at[jj])
        for d in (2, 3, 1, 0):
            part = slice(512 + d * 128, 512 + (d + 1) * 128)
            here = slice(d * 128, (d + 1) * 128)
            v = both(jj, 1, o, part)
            if o == 0:
                v = v + rx1[jj, 1, here, :].astype(F32) + ry2[jj, here, :].astype(F32)
            else:
                v = v + ry1[jj, part, :].astype(F32) + rx2[jj, here, :].astype(F32)
            if d:
                s3[jj, o, d - 1] = v.astype(BF16)
                send(("rz", jj, o, d), s3.at[jj, o, d - 1], rz.at[jj, o, d - 1], z_peer[d])
            else:
                keep[jj, o] = v

    def final(jj, o):
        v = keep[jj, o]
        for d in (1, 2, 3):
            got(("rz", jj, o, d), rz.at[jj, o, d - 1])
            v = v + rz[jj, o, d - 1].astype(F32)
        at = jj * 256 + o * 128
        moe_out[:, at : at + 128] = v.astype(BF16)

    need("ag", "tf", "fine", "coarse")
    qkv(3)

    @pl.when(me < n_ep - 1)
    def _():
        copy("halo", halo_s, halo_r, {"ep": (me + 1) % n_ep, "tp": t}).start()

    arrived("z", R(1, 1), 1)
    to_x(1)
    to_core(R(1, 1), 1)
    arrived("x", R(0, 0), 1)
    to_core(R(0, 0), 1)
    qkv(0)
    qkv(1)
    arrived("z", R(2, 1), 1)
    to_x(2)
    to_y(R(2, 1))
    to_core(R(2, 1), 1)
    arrived("x", R(0, 0), 0)
    to_core(R(0, 0), 0)
    qkv(2)
    onehots()
    arrived("z", R(3, 1), 1)
    to_x(3)
    to_y(R(3, 1))
    to_core(R(3, 1), 1)
    arrived("z", R(1, 1), 0)
    to_core(R(1, 1), 0)
    attend(1)
    arrived("x", R(1, 0), 1)
    to_y(R(1, 0))
    to_core(R(1, 0), 1)
    attend(2)
    arrived("x", R(2, 0), 1)
    to_y(R(2, 0))
    to_core(R(2, 0), 1)
    attend(3)

    @pl.when(me == 0)
    def _():
        halo_r[...] = jnp.zeros_like(halo_r)

    @pl.when(me > 0)
    def _():
        got("halo", halo_r)

    store_kv(halo_r[:, 0:128].astype(F32), halo_r[:, 128:256].astype(F32), 0)
    attend(0)
    arrived("x", R(3, 0), 1)
    to_y(R(3, 0))
    to_core(R(3, 0), 1)
    for k in (0, 1):
        send(("mrc", k), mp.at[ysel[k] * 2 + 1 - c], mrc.at[k], c_peer)
    shared_hidden()
    from_y(R(2, 1))
    from_y(R(3, 1))
    got(("mrc", 0), mrc.at[0])
    ms[...] = (mp[ysel[0] * 2 + c].astype(F32) + mrc[0].astype(F32)).astype(BF16)
    send("mry", ms, mry, y_peer)
    from_y(R(1, 0))
    first = (R(0, 1), R(0, 0), R(1, 1), R(1, 0))
    second = (R(2, 1), R(3, 1), R(2, 0), R(3, 0))
    for r in first[1:]:
        from_core(r)
    dispatch(0, first)
    gate_up(0, first, 0)
    from_y(R(2, 0))
    gate_up(0, first, 1)
    from_y(R(3, 0))
    to_tokens(first)
    for r in second:
        from_core(r)
    dispatch(1, second)
    gate_up(1, second, 0)
    gate_up(1, second, 1)
    to_tokens(second)
    for jj in range(2):
        for yr in range(2):
            down(jj, yr, mo_peer, 1 - c)
        core_send(jj)
        for yr in range(2):
            down(jj, yr, mo_own, c)
        stage1(jj)
    stage2(0)
    got(("mrc", 1), mrc.at[1])
    got("mry", mry)
    mix_out[...] = (
        mp[ysel[1] * 2 + c].astype(F32) + mrc[1].astype(F32) + mry[...].astype(F32)
    ).astype(BF16)
    stage3(0, 0)
    stage3(0, 1)
    stage2(1)
    final(0, 0)
    final(0, 1)
    stage3(1, 0)
    stage3(1, 1)
    final(1, 0)
    final(1, 1)

    @pl.when(me < n_ep - 1)
    def _():
        copy("halo", halo_s, halo_r, {"ep": (me + 1) % n_ep, "tp": t}).wait_send()

    for k in started:
        k.wait_send()
    assert not loads and len(ids) <= ss.shape[0]


def rope_tables(tokens, rows):
    freqs = rope_base ** (-np.arange(0, HEAD_SIZE, 2) / HEAD_SIZE)
    freqs = np.tile(freqs, 128 // len(freqs))
    fine = np.arange(rows)[:, None] * freqs[None, :]
    coarse = np.arange(0, tokens, rows)[:, None] * freqs[None, :]
    return [
        jnp.asarray(np.stack([np.cos(a), np.sin(a)]), dtype=jnp.float32) for a in (fine, coarse)
    ]


def fused(tf, ag, wq, wk, wv, sink, wo, ts, fg, routes, rweight, wg, wu, wd, sg, su, sd):
    n_ep = lax.axis_size("ep")
    rows, wide = ts.shape
    exp_dev, _, hidden = wg.shape
    cap = max(2, 2 * rows * routes.shape[1] // (exp_dev * n_ep))
    mrows = tf.shape[0] // 4
    fine, coarse = rope_tables(tf.shape[0] * n_ep, rows)
    args = (
        sink, ag.reshape(1, -1), fg.reshape(1, -1), routes.T, rweight.T, fine, coarse,
        tf, wq, wk, wv, wo, ts, wg, wu, wd, sg, su, sd,
    )
    vm = pl.BlockSpec(memory_space=pltpu.VMEM)
    hbm = pl.BlockSpec(memory_space=pl.ANY)
    v = pltpu.VMEM
    dma = pltpu.SemaphoreType.DMA
    qw = wide // 4
    scratch = [v(a.shape, a.dtype) for a in args[1:]] + [
        v((tf.shape[0], 256), BF16),
        v((2, tf.shape[0] + rows, 128), BF16),
        v((2, tf.shape[0] + rows, 128), BF16),
        v((rows, 256), BF16),
        v((rows, 256), BF16),
        v((n_ep, 4, rows, qw), BF16),
        v((n_ep, 2 * routes.shape[1], rows), F32),
        v((n_ep, exp_dev * cap, rows), BF16),
        v((n_ep, exp_dev, rows, exp_dev * cap), BF16),
        v((n_ep, exp_dev, cap, 1), F32),
        v((exp_dev, n_ep * cap, wide), BF16),
        v((n_ep * exp_dev * cap, hidden), BF16),
        v((n_ep * rows, exp_dev * hidden), BF16),
        v((rows, sg.shape[1]), BF16),
        v((4, mrows, wide), BF16),
        v((2, mrows, wide), BF16),
        v((mrows, wide), BF16),
        v((mrows, wide), BF16),
        v((2, 2, 2, n_ep * rows, 128), BF16),
        v((2, 2, 2, n_ep * rows, 128), BF16),
        v((2, 2, 2, n_ep * rows, 128), BF16),
        v((2, 2, 4 * rows, 128), BF16),
        v((2, 2, 4 * rows, 128), BF16),
        v((2, 8 * rows, 128), BF16),
        v((2, 8 * rows, 128), BF16),
        v((2, 4 * rows, 128), BF16),
        v((2, 4 * rows, 128), BF16),
        v((2, 4 * rows, 128), BF16),
        v((2, 4 * rows, 128), BF16),
        v((2, 2, 3, rows, 128), BF16),
        v((2, 2, 3, rows, 128), BF16),
        v((2, 2, rows, 128), F32),
        dma((18,)), dma((72,)), dma((72,)),
    ]
    moe_out_shape = jax.ShapeDtypeStruct((rows, qw), BF16)
    mix_out_shape = jax.ShapeDtypeStruct((mrows, wide), BF16)
    return pl.pallas_call(
        functools.partial(fused_kernel, cap),
        out_shape=(mix_out_shape, moe_out_shape),
        in_specs=[pl.BlockSpec(memory_space=pltpu.SMEM)] + [hbm] * (len(args) - 1),
        out_specs=(vm, vm),
        scratch_shapes=scratch,
        compiler_params=pltpu.CompilerParams(
            collective_id=0, has_side_effects=True, vmem_limit_bytes=60 * 1024 * 1024
        ),
        name="fused",
    )(*args)


def local(
    tokens_first,
    attn_gain,
    w_query,
    key_matrix,
    value_matrix,
    head_sink_logit,
    w_output,
    tokens_second,
    ffn_gain,
    routes,
    route_weight,
    w_gate_exp,
    w_up_exp,
    w_down_exp,
    w_gate_shared,
    w_up_shared,
    w_down_shared,
):
    if lax.axis_size("ep") == 8 and lax.axis_size("tp") == 4:
        return fused(
            tokens_first, attn_gain, w_query, key_matrix, value_matrix, head_sink_logit, w_output,
            tokens_second, ffn_gain, routes, route_weight, w_gate_exp, w_up_exp, w_down_exp,
            w_gate_shared, w_up_shared, w_down_shared,
        )
    rows_first = tokens_first.shape[0]
    norm_input = rms_scale(tokens_first, attn_gain)
    offset = lax.axis_index("ep") * rows_first
    token_positions = (offset + jnp.arange(rows_first, dtype=jnp.int32)).astype(jnp.float32)
    head_count = w_query.shape[1] // HEAD_SIZE
    key_heads = key_matrix.shape[1] // HEAD_SIZE
    head_group = head_count // key_heads
    query_rows = apply_rotary(
        jnp.dot(norm_input, w_query, preferred_element_type=jnp.float32).reshape(
            rows_first, head_count, HEAD_SIZE
        ),
        token_positions,
    ).astype(jnp.bfloat16)
    keys_local = apply_rotary(
        jnp.dot(norm_input, key_matrix, preferred_element_type=jnp.float32).reshape(
            rows_first, key_heads, HEAD_SIZE
        ),
        token_positions,
    ).astype(jnp.bfloat16)
    values_local = (
        jnp.dot(norm_input, value_matrix, preferred_element_type=jnp.float32)
        .astype(jnp.bfloat16)
        .reshape(rows_first, key_heads, HEAD_SIZE)
    )
    keys_before, values_before = from_behind(
        (keys_local[rows_first - BAND_LENGTH :], values_local[rows_first - BAND_LENGTH :]),
        "ep",
        1,
    )
    keys_all = jnp.concatenate([keys_before, keys_local], axis=0)
    values_all = jnp.concatenate([values_before, values_local], axis=0)
    band = BAND_LENGTH
    bands = rows_first // band

    def windows(padded):
        return jnp.concatenate(
            [
                padded[:rows_first].reshape(bands, band, key_heads, HEAD_SIZE),
                padded[band:].reshape(bands, band, key_heads, HEAD_SIZE),
            ],
            axis=1,
        )

    sink_scores = head_sink_logit.reshape(key_heads, head_group)[None, :, :, None, None]
    scores = jnp.einsum(
        "bqhgd,bkhd->bhgqk",
        query_rows.reshape(bands, band, key_heads, head_group, HEAD_SIZE),
        windows(keys_all),
        preferred_element_type=jnp.float32,
    ) * HEAD_SIZE ** (-0.5)
    offsets = (
        band
        + jnp.arange(band, dtype=jnp.int32)[:, None]
        - jnp.arange(2 * band, dtype=jnp.int32)[None, :]
    )
    key_pos = (
        offset
        + (jnp.arange(bands, dtype=jnp.int32)[:, None] - 1) * band
        + jnp.arange(2 * band, dtype=jnp.int32)[None, :]
    )
    visible = ((offsets >= 0) & (offsets < band))[None] & (key_pos >= 0)[:, None, :]
    scores = jnp.where(visible[:, None, None], scores, -jnp.inf)
    peak = jnp.maximum(jnp.max(scores, axis=-1, keepdims=True), sink_scores)
    expo = jnp.exp(scores - peak)
    total = jnp.sum(expo, axis=-1, keepdims=True) + jnp.exp(sink_scores - peak)
    weights = (expo / total).astype(jnp.bfloat16)
    attended = (
        jnp.einsum(
            "bhgqk,bkhd->bqhgd", weights, windows(values_all), preferred_element_type=jnp.float32
        )
        .astype(jnp.bfloat16)
        .reshape(rows_first, head_count * HEAD_SIZE)
    )
    mixer_out = lax.psum_scatter(
        jnp.dot(attended, w_output, preferred_element_type=jnp.float32).astype(jnp.bfloat16),
        "tp",
        scatter_dimension=0,
        tiled=True,
    )
    rows_second = tokens_second.shape[0]
    topk = routes.shape[1]
    exp_dev = w_gate_exp.shape[0]
    n_expdev = lax.axis_size("ep")
    experts = exp_dev * n_expdev
    capacity = max(2, 2 * rows_second * topk // experts)
    slot_count = experts * capacity
    normed_second = rms_scale(tokens_second, ffn_gain)
    flat = routes.reshape(-1)
    onehot = (flat[:, None] == jnp.arange(experts, dtype=jnp.int32)[None, :]).astype(jnp.int32)
    ranks = jnp.sum((jnp.cumsum(onehot, axis=0) - onehot) * onehot, axis=1)
    slots = flat * capacity + ranks
    match = (jnp.arange(slot_count, dtype=jnp.int32)[:, None] == slots[None, :]).reshape(
        slot_count, rows_second, topk
    )
    dispatch = jnp.sum(match.astype(jnp.float32), axis=2).astype(jnp.bfloat16)
    combine = jnp.sum(match.astype(jnp.float32) * route_weight[None, :, :], axis=2)
    width = normed_second.shape[1] // lax.axis_size("tp")
    feature_slice = lax.dynamic_slice_in_dim(normed_second, lax.axis_index("tp") * width, width, 1)
    outgoing = jnp.dot(dispatch, feature_slice, preferred_element_type=jnp.float32).astype(
        jnp.bfloat16
    )
    arrived = lax.all_to_all(outgoing, "ep", split_axis=0, concat_axis=0, tiled=True)
    piece = lax.all_gather(arrived, "tp", axis=1, tiled=True)
    cols = piece.shape[1]
    part = piece.reshape(n_expdev, exp_dev, capacity, cols)
    gate_pre = jnp.einsum("sjcd,jdf->sjcf", part, w_gate_exp, preferred_element_type=jnp.float32)
    up_pre = jnp.einsum("sjcd,jdf->sjcf", part, w_up_exp, preferred_element_type=jnp.float32)
    hidden = (jax.nn.silu(gate_pre) * up_pre).astype(jnp.bfloat16)
    shared_hidden = (
        jax.nn.silu(jnp.dot(normed_second, w_gate_shared, preferred_element_type=jnp.float32))
        * jnp.dot(normed_second, w_up_shared, preferred_element_type=jnp.float32)
    ).astype(jnp.bfloat16)
    routed_term = jnp.einsum(
        "sjcf,jfd->dsjc", hidden, w_down_exp, preferred_element_type=jnp.float32
    ).reshape(lax.axis_size("tp") * (MODEL_WIDTH // lax.axis_size("tp")), slot_count)
    shared_term = lax.dot_general(
        w_down_shared, shared_hidden, (((0,), (1,)), ((), ())), preferred_element_type=jnp.float32
    )
    summed = lax.psum_scatter(
        jnp.concatenate([routed_term, shared_term], axis=1).astype(jnp.bfloat16),
        "tp",
        scatter_dimension=0,
        tiled=True,
    ).astype(jnp.float32)
    routed_part = summed[:, :slot_count].astype(jnp.bfloat16)
    returned = lax.all_to_all(routed_part, "ep", split_axis=1, concat_axis=1, tiled=True)
    weighted = lax.dot_general(
        combine,
        returned.astype(jnp.float32),
        (((0,), (1,)), ((), ())),
        precision=lax.Precision.HIGHEST,
    )
    moe_out = (weighted + summed[:, slot_count:].T).astype(jnp.bfloat16)
    return (mixer_out, moe_out)


def solution(mesh):
    in_specs = (
        P("ep", None),
        P(),
        P(None, "tp"),
        P(None, "tp"),
        P(None, "tp"),
        P("tp"),
        P("tp", None),
        P("ep", None),
        P(),
        P("ep", None),
        P("ep", None),
        P("ep", None, "tp"),
        P("ep", None, "tp"),
        P("ep", "tp", None),
        P(None, "tp"),
        P(None, "tp"),
        P("tp", None),
    )
    out_specs = (P(("ep", "tp"), None), P("ep", "tp"))
    return jax.shard_map(local, mesh=mesh, in_specs=in_specs, out_specs=out_specs, check_vma=False)
```

```python
import functools
import jax
import jax.numpy as jnp
import numpy as np
from jax import lax
from jax.experimental import pallas as pl
from jax.experimental.pallas import tpu as pltpu
from jax.sharding import PartitionSpec as P

MODEL_WIDTH = 2048
HEAD_SIZE = 64
BAND_LENGTH = 128


rope_base = 10000.0
norm_eps = 1e-06


def from_behind(value, axis, by):
    devices = lax.axis_size(axis)
    pairs = [(i, i + by) for i in range(devices) if 0 <= i + by < devices]
    return lax.ppermute(value, axis, pairs)


def rms_scale(inputs, gain):
    wide = inputs.astype(jnp.float32)
    scaled = wide * lax.rsqrt(jnp.mean(wide * wide, axis=-1, keepdims=True) + norm_eps)
    return (scaled * gain).astype(jnp.bfloat16)


def apply_rotary(heads, token_positions):
    freqs = rope_base ** (-jnp.arange(0, HEAD_SIZE, 2, dtype=jnp.float32) / HEAD_SIZE)
    angles = token_positions[:, None] * freqs[None, :]
    cosine = jnp.cos(angles)[:, None, :]
    sine = jnp.sin(angles)[:, None, :]
    first_half, second_half = jnp.split(heads, 2, axis=-1)
    return jnp.concatenate(
        [first_half * cosine - second_half * sine, second_half * cosine + first_half * sine],
        axis=-1,
    )


MESH = pl.DeviceIdType.MESH
F32 = jnp.float32
BF16 = jnp.bfloat16


def dot(a, b):
    return jnp.dot(a, b, preferred_element_type=F32)


def scoped(f):
    def call(*a):
        with jax.named_scope("_".join([f.__name__] + [str(v) for v in a if isinstance(v, int)])):
            return f(*a)

    return call


def lanes_of(shape):
    return lax.broadcasted_iota(jnp.int32, shape, len(shape) - 1)


def fused_kernel(
    cap,
    sinks, ag_h, fg_h, rt_h, rw_h, fine_h, coarse_h, tf_h, wq_h, wk_h, wv_h, wo_h, ts_h,
    wg_h, wu_h, wd_h, sg_h, su_h, sd_h,
    mix_out, moe_out,
    ag, fg, rt, rw, fine, coarse, tf, wq, wk, wv, wo, ts, wg, wu, wd, sg, su, sd,
    qs, kd, vd, halo_s, halo_r, xg, mg, oh, oht, wsl, xs, hid, tokh, shh,
    mp, mrc, ms, mry, mo_own, mo_peer, rc, s1x, rx1, s2y, ry2, s3, rz, keep,
    lsem, ss, rs,
):
    me, t = lax.axis_index("ep"), lax.axis_index("tp")
    z, x, y, c = me // 2, me % 2, t // 2, t % 2
    zs = (z, z + 1 - 2 * (z % 2), (z + 2) % 4, 3 - z)
    z_peer = [{"ep": zd * 2 + x, "tp": t} for zd in zs]
    x_peer = {"ep": z * 2 + 1 - x, "tp": t}
    y_peer = {"ep": me, "tp": (1 - y) * 2 + c}
    c_peer = {"ep": me, "tp": y * 2 + 1 - c}
    n_ep = 8
    exp_dev = wg.shape[0]
    topk = rt.shape[0]
    rows = ts.shape[0]
    blocks = tf.shape[0] // rows

    loads = {}

    def load(name, src, dst):
        k = pltpu.make_async_copy(src, dst, lsem.at[len(loads)])
        k.start()
        loads[name] = k

    def need(*names):
        for name in names:
            k = loads.pop(name, None)
            if k is not None:
                done.append(name)
                k.wait()

    done = []
    pairs = [
        ("ts", ts_h, ts), ("fg", fg_h, fg), ("rt", rt_h, rt), ("rw", rw_h, rw), ("ag", ag_h, ag),
        ("tf", tf_h, tf), ("fine", fine_h, fine), ("coarse", coarse_h, coarse), ("wq", wq_h, wq),
        ("wk", wk_h, wk), ("wv", wv_h, wv), ("wo", wo_h, wo), ("sg", sg_h, sg), ("su", su_h, su),
        ("wg", wg_h, wg), ("wu", wu_h, wu), ("wd", wd_h, wd), ("sd", sd_h, sd),
    ]
    for name, a, b in pairs:
        load(name, a, b)

    barrier = pltpu.get_barrier_semaphore()
    for e in range(1, n_ep):
        pl.semaphore_signal(
            barrier, inc=1, device_id={"ep": (me + e) % n_ep, "tp": t}, device_id_type=MESH
        )
    for peer in (y_peer, c_peer):
        pl.semaphore_signal(barrier, inc=1, device_id=peer, device_id_type=MESH)

    ids = {}
    started = []

    def copy(name, src, dst, peer):
        i = ids.setdefault(name, len(ids))
        return pltpu.make_async_remote_copy(
            src_ref=src, dst_ref=dst, send_sem=ss.at[i], recv_sem=rs.at[i],
            device_id=peer, device_id_type=MESH,
        )

    def send(name, src, dst, peer):
        k = copy(name, src, dst, peer)
        k.start()
        started.append(k)

    def got(name, dst):
        copy(name, dst, dst, c_peer).wait_recv()

    def normed(wide, gain):
        return (
            wide * lax.rsqrt(jnp.mean(wide * wide, axis=-1, keepdims=True) + norm_eps) * gain
        ).astype(BF16)

    turn = (0, 3, 1, 2)

    def R(d, s):
        return turn[d] * 2 + s

    own = R(0, 1)
    quarter = xg.shape[3]

    def q_of(k, cc):
        return (y if k else 1 - y) * 2 + cc

    @scoped
    def norm_second():
        need("ts", "fg", "rt", "rw")
        xn = normed(ts[...].astype(F32), fg[...])
        for q in range(4):
            xg[own, q] = xn[:, q * quarter : (q + 1) * quarter]
        mg[own] = jnp.concatenate([rt[...].astype(F32), rw[...]], axis=0)

    norm_second()

    @scoped
    def barrier_wait():
        pl.semaphore_wait(barrier, n_ep + 1)

    barrier_wait()

    for s in (0, 1):
        for d in range(4):
            if R(d, s) != own:
                peer = {"ep": zs[d] * 2 + (x if s else 1 - x), "tp": t}
                send(("m", R(d, s)), mg.at[own], mg.at[R(d, s)], peer)

    parts = 2
    sub = rows // parts

    def piece(at, q, p):
        return xg.at[at, q, p * sub : (p + 1) * sub, :]

    def block_send(link, k, peer, at, p):
        q = q_of(k, c)
        send((link, at, k, p), piece(own, q, p), piece(at, q, p), peer)

    for p in range(parts):
        block_send("z", 1, z_peer[2], R(2, 1), p)
        block_send("x", 1, x_peer, R(0, 0), p)
    for p in range(parts):
        block_send("z", 1, z_peer[3], R(3, 1), p)
        block_send("x", 0, x_peer, R(0, 0), p)
    for p in range(parts):
        block_send("z", 1, z_peer[1], R(1, 1), p)
        block_send("z", 0, z_peer[1], R(1, 1), p)

    def arrive(link, d, s, k, p, *onward):
        at, q = R(d, s), q_of(k, c)
        here = piece(at, q, p)
        with jax.named_scope("%s_d%d_s%d_k%d_p%d" % (link, d, s, k, p)):
            got((link, at, k, p), here)
        for way in onward:
            if way == "x":
                send(("x", R(d, 0), k, p), here, piece(R(d, 0), q, p), x_peer)
            else:
                send(("y", at, 0, p), here, here, y_peer)
        send(("c", at, k, p), here, here, c_peer)

    @scoped
    def from_core(at):
        for p in range(parts):
            for k in (1, 0):
                got(("c", at, k, p), piece(at, q_of(k, 1 - c), p))

    lane = lanes_of((rows, 128))
    low = lane % 64 < 32
    left = lane < 64

    @scoped
    def qkv(b):
        part = slice(b * rows, (b + 1) * rows)
        nb = normed(tf[part].astype(F32), ag[...])
        base = pl.ds(me * blocks + b, 1)
        cb, sb = coarse[0, base, :], coarse[1, base, :]
        cosine = fine[0] * cb - fine[1] * sb
        sine = fine[1] * cb + fine[0] * sb
        sine = jnp.where(low, -sine, sine)

        def rot(v):
            swap = jnp.where(low, pltpu.roll(v, 96, 1), pltpu.roll(v, 32, 1))
            return v * cosine + swap * sine

        need("wk")
        kk = rot(dot(nb, wk[...]))
        need("wv")
        vv = dot(nb, wv[...])
        store_kv(kk.astype(BF16).astype(F32), vv.astype(BF16).astype(F32), (b + 1) * rows)
        if b == blocks - 1:
            halo_s[:, 0:128] = kk.astype(BF16)
            halo_s[:, 128:256] = vv.astype(BF16)
        need("wq")
        for g in range(2):
            qq = rot(dot(nb, wq[:, g * 128 : (g + 1) * 128])) * HEAD_SIZE ** (-0.5)
            qs[part, g * 128 : (g + 1) * 128] = qq.astype(BF16)

    def store_kv(kk, vv, at):
        for ref, val in ((kd, kk), (vd, vv)):
            other = pltpu.roll(val, 64, 1)
            ref[0, at : at + rows, :] = jnp.where(left, val, other).astype(BF16)
            ref[1, at : at + rows, :] = jnp.where(left, other, val).astype(BF16)

    i2 = lax.broadcasted_iota(jnp.int32, (2 * rows, 2 * rows), 0)
    band = lanes_of((2 * rows, 2 * rows)) - i2 % rows
    top = lax.broadcasted_iota(jnp.int32, (2 * rows, 1), 0) < rows

    @scoped
    def attend(b):
        part = slice(b * rows, (b + 1) * rows)
        outs = []
        visible = (band > 0) & (band <= rows)
        if b == 0:
            visible = visible & ((lanes_of((2 * rows, 2 * rows)) >= rows) | (me > 0))
        for g in range(2):
            q2 = qs[part, g * 128 : (g + 1) * 128]
            zero = jnp.zeros_like(q2)
            qq = jnp.concatenate([jnp.where(left, q2, zero), jnp.where(left, zero, q2)], axis=0)
            score = lax.dot_general(
                qq, kd[g, b * rows : (b + 2) * rows, :], (((1,), (1,)), ((), ())),
                preferred_element_type=F32,
            )
            score = jnp.where(visible, score, -jnp.inf)
            sink = jnp.where(top, sinks[2 * g], sinks[2 * g + 1])
            peak = jnp.maximum(jnp.max(score, axis=-1, keepdims=True), sink)
            expo = jnp.exp(score - peak)
            total = jnp.sum(expo, axis=-1, keepdims=True) + jnp.exp(sink - peak)
            weights = (expo * (1.0 / total)).astype(BF16)
            o = dot(weights, vd[g, b * rows : (b + 2) * rows, :])
            outs.append(jnp.where(left, o[:rows], o[rows:]).astype(BF16))
        att = jnp.concatenate(outs, axis=1)
        need("wo")
        for n in range(4):
            mp[b, :, n * 512 : (n + 1) * 512] = dot(att, wo[:, n * 512 : (n + 1) * 512]).astype(BF16)

    @scoped
    def onehots():
        for s in (0, 1):
            for d in range(4):
                if R(d, s) != own:
                    got(("m", R(d, s)), mg.at[R(d, s)])
        before = (
            lax.broadcasted_iota(jnp.int32, (rows, rows), 0)
            < lax.broadcasted_iota(jnp.int32, (rows, rows), 1)
        ).astype(F32).astype(BF16)
        hits, vals = [], []
        for r in range(n_ep):
            for e in range(exp_dev):
                named = mg[r, 0:topk, :] == (me * exp_dev + e).astype(F32)
                hits.append(jnp.sum(named.astype(F32), axis=0, keepdims=True))
                vals.append(
                    jnp.sum(jnp.where(named, mg[r, topk : 2 * topk, :], 0.0), axis=0, keepdims=True)
                )
        ranks = dot(jnp.concatenate(hits, axis=0).astype(BF16), before)
        slot = lax.broadcasted_iota(jnp.int32, (cap, rows), 0).astype(F32)
        for r in range(n_ep):
            both = []
            for e in range(exp_dev):
                i = r * exp_dev + e
                at = (slot == ranks[i : i + 1, :]) & (hits[i] > 0.0)
                both.append(at.astype(F32))
                wsl[r, e] = jnp.sum(jnp.where(at, vals[i], 0.0), axis=1, keepdims=True)
            full = jnp.concatenate(both, axis=0)
            oh[r] = full.astype(BF16)
            turned = full.T
            for e in range(exp_dev):
                oht[r, e] = jnp.where(lanes_of(turned.shape) // cap == e, turned, 0.0).astype(BF16)

    @scoped
    def shared_hidden():
        need("sg", "su")
        g = jnp.zeros((rows, sg.shape[1]), F32)
        u = jnp.zeros((rows, sg.shape[1]), F32)
        for q in range(4):
            part = slice(q * quarter, (q + 1) * quarter)
            g = g + dot(xg[own, q], sg[part, :])
            u = u + dot(xg[own, q], su[part, :])
        shh[...] = (g / (1.0 + jnp.exp(-g)) * u).astype(BF16)

    def pair(d):
        return (R(d, 0), R(d, 1))

    @scoped
    def dispatch(d):
        for i, r in enumerate(pair(d)):
            for q in range(4):
                v = dot(oh[r], xg[r, q]).astype(BF16)
                for e in range(exp_dev):
                    xs[e, i * cap : (i + 1) * cap, q * quarter : (q + 1) * quarter] = v[
                        e * cap : (e + 1) * cap
                    ]

    @scoped
    def gate_up(d, e):
        need("wg", "wu")
        wcol = jnp.concatenate([wsl[r, e] for r in pair(d)], axis=0)
        for n in range(hid.shape[1] // 256):
            cs = slice(n * 256, (n + 1) * 256)
            g = dot(xs[e], wg[e, :, cs])
            u = dot(xs[e], wu[e, :, cs])
            hh = (g / (1.0 + jnp.exp(-g)) * u * wcol).astype(BF16)
            for i, r in enumerate(pair(d)):
                hid[r * rows + e * cap : r * rows + (e + 1) * cap, cs] = hh[i * cap : (i + 1) * cap]

    @scoped
    def to_tokens(d):
        width = hid.shape[1]
        for r in pair(d):
            for e in range(exp_dev):
                tokh[r * rows : (r + 1) * rows, e * width : (e + 1) * width] = dot(
                    oht[r, e], hid[r * rows : (r + 1) * rows, :]
                ).astype(BF16)

    ysel = (1 - y, y)

    @scoped
    def down(d, yr, peer):
        need("wd", "sd")
        i = turn[d]
        cc = 1 - c if peer else c
        out = mo_peer if peer else mo_own
        width = hid.shape[1]
        part = slice(i * 256, (i + 1) * 256)
        for n in range(2):
            base = pl.multiple_of((ysel[yr] * 2 + cc) * 512 + n * 256, 256)
            cs = pl.ds(base, 256)
            v = dot(tokh[part, 0:width], wd[0, :, cs]) + dot(tokh[part, width : 2 * width], wd[1, :, cs])
            if d == 0:
                v = jnp.concatenate([v[:rows], v[rows:] + dot(shh[...], sd[:, cs])], axis=0)
            out[i, yr, :, n * 256 : (n + 1) * 256] = v.astype(BF16)
        if peer:
            send(("rc", i, yr), mo_peer.at[i, yr], rc.at[i, yr], c_peer)

    def both(i, yr, part):
        return mo_own[i, yr, part, :].astype(F32) + rc[i, yr, part, :].astype(F32)

    far, near = slice(0, 128), slice(128, 256)

    @scoped
    def stage1(d, yr):
        i = turn[d]
        got(("rc", i, yr), rc.at[i, yr])
        s1x[i, yr] = both(i, yr, far).astype(BF16)
        send(("rx1", i, yr), s1x.at[i, yr], rx1.at[i, yr], x_peer)

    @scoped
    def stage2(d):
        i = turn[d]
        got(("rx1", i, 0), rx1.at[i, 0])
        s2y[i] = (both(i, 0, near) + rx1[i, 0].astype(F32)).astype(BF16)
        send(("ry2", i), s2y.at[i], ry2.at[i], y_peer)

    @scoped
    def stage3(d):
        i = turn[d]
        got(("rx1", i, 1), rx1.at[i, 1])
        v = both(i, 1, near) + rx1[i, 1].astype(F32)
        got(("ry2", i), ry2.at[i])
        v = v + ry2[i].astype(F32)
        if d:
            s3[d - 1] = v.astype(BF16)
            send(("rz", d), s3.at[d - 1], rz.at[d - 1], z_peer[d])
        else:
            keep[...] = v

    @scoped
    def final():
        v = keep[...]
        for d in (2, 3, 1):
            got(("rz", d), rz.at[d - 1])
            v = v + rz[d - 1].astype(F32)
        moe_out[...] = v.astype(BF16)

    @scoped
    def mixer_sum():
        got(("mrc", 0), mrc.at[0])
        ms[...] = (mp[ysel[0] * 2 + c].astype(F32) + mrc[0].astype(F32)).astype(BF16)

    def mixer_send():
        send("mry", ms, mry, y_peer)

    @scoped
    def mixer_final():
        got(("mrc", 1), mrc.at[1])
        got("mry", mry)
        mix_out[...] = (
            mp[ysel[1] * 2 + c].astype(F32) + mrc[1].astype(F32) + mry[...].astype(F32)
        ).astype(BF16)

    @scoped
    def halo_in():
        @pl.when(me == 0)
        def _():
            halo_r[...] = jnp.zeros_like(halo_r)

        @pl.when(me > 0)
        def _():
            got("halo", halo_r)

        store_kv(halo_r[:, 0:128].astype(F32), halo_r[:, 128:256].astype(F32), 0)

    need("ag", "tf", "fine", "coarse")
    qkv(3)

    @pl.when(me < n_ep - 1)
    def _():
        copy("halo", halo_s, halo_r, {"ep": (me + 1) % n_ep, "tp": t}).start()

    def cores(d):
        for r in pair(d):
            if r != own:
                from_core(r)

    qkv(0)
    qkv(1)
    arrive("x", 0, 0, 1, 0)
    arrive("x", 0, 0, 1, 1)
    qkv(2)
    arrive("z", 2, 1, 1, 0, "y", "x")
    arrive("x", 0, 0, 0, 0)
    onehots()
    arrive("x", 0, 0, 0, 1)
    attend(1)
    arrive("z", 2, 1, 1, 1, "y", "x")
    shared_hidden()
    attend(2)
    arrive("y", 2, 1, 0, 0)
    arrive("x", 2, 0, 1, 0, "y")
    cores(0)
    dispatch(0)
    gate_up(0, 0)
    arrive("z", 3, 1, 1, 0, "x", "y")
    arrive("y", 2, 1, 0, 1)
    gate_up(0, 1)
    to_tokens(0)
    arrive("x", 2, 0, 1, 1, "y")
    down(0, 0, True)
    down(0, 1, True)
    arrive("y", 2, 0, 0, 0)
    arrive("z", 1, 1, 1, 0, "x")
    arrive("z", 3, 1, 1, 1, "x", "y")
    down(0, 0, False)
    down(0, 1, False)
    attend(3)
    arrive("z", 1, 1, 0, 0, "x")
    arrive("x", 3, 0, 1, 0, "y")
    arrive("y", 3, 1, 0, 0)
    halo_in()
    attend(0)
    for k in (0, 1):
        send(("mrc", k), mp.at[ysel[k] * 2 + 1 - c], mrc.at[k], c_peer)
    arrive("y", 2, 0, 0, 1)
    arrive("z", 1, 1, 1, 1, "x")
    mixer_sum()
    cores(2)
    dispatch(2)
    arrive("z", 1, 1, 0, 1, "x")
    stage1(0, 1)
    arrive("x", 3, 0, 1, 1, "y")
    mixer_send()
    arrive("y", 3, 1, 0, 1)
    gate_up(2, 0)
    arrive("x", 1, 0, 1, 0)
    arrive("x", 1, 0, 0, 0)
    arrive("y", 3, 0, 0, 0)
    gate_up(2, 1)
    arrive("x", 1, 0, 1, 1)
    to_tokens(2)
    down(2, 0, True)
    down(2, 1, True)
    arrive("x", 1, 0, 0, 1)
    arrive("y", 3, 0, 0, 1)
    down(2, 0, False)
    stage1(2, 0)
    down(2, 1, False)
    stage1(2, 1)
    cores(3)
    dispatch(3)
    gate_up(3, 0)
    gate_up(3, 1)
    to_tokens(3)
    down(3, 0, True)
    down(3, 1, True)
    down(3, 0, False)
    stage1(3, 0)
    down(3, 1, False)
    stage1(3, 1)
    stage2(2)
    cores(1)
    dispatch(1)
    gate_up(1, 0)
    gate_up(1, 1)
    to_tokens(1)
    down(1, 0, True)
    down(1, 1, True)
    down(1, 0, False)
    stage1(1, 0)
    stage1(0, 0)
    down(1, 1, False)
    stage1(1, 1)
    stage2(3)
    stage3(2)
    stage2(1)
    stage2(0)
    stage3(3)
    mixer_final()
    stage3(1)
    stage3(0)
    final()

    @pl.when(me < n_ep - 1)
    def _():
        copy("halo", halo_s, halo_r, {"ep": (me + 1) % n_ep, "tp": t}).wait_send()

    @scoped
    def all_sent():
        for k in started:
            k.wait_send()

    all_sent()
    assert not loads and len(ids) <= ss.shape[0]


def rope_tables(tokens, rows):
    freqs = rope_base ** (-np.arange(0, HEAD_SIZE, 2) / HEAD_SIZE)
    freqs = np.tile(freqs, 128 // len(freqs))
    fine = np.arange(rows)[:, None] * freqs[None, :]
    coarse = np.arange(0, tokens, rows)[:, None] * freqs[None, :]
    return [
        jnp.asarray(np.stack([np.cos(a), np.sin(a)]), dtype=jnp.float32) for a in (fine, coarse)
    ]


def fused(tf, ag, wq, wk, wv, sink, wo, ts, fg, routes, rweight, wg, wu, wd, sg, su, sd):
    n_ep = lax.axis_size("ep")
    rows, wide = ts.shape
    exp_dev, _, hidden = wg.shape
    cap = max(2, 2 * rows * routes.shape[1] // (exp_dev * n_ep))
    mrows = tf.shape[0] // 4
    fine, coarse = rope_tables(tf.shape[0] * n_ep, rows)
    args = (
        sink, ag.reshape(1, -1), fg.reshape(1, -1), routes.T, rweight.T, fine, coarse,
        tf, wq, wk, wv, wo, ts, wg, wu, wd, sg, su, sd,
    )
    args = tuple(pltpu.with_memory_space_constraint(a, pltpu.HBM) for a in args)
    vm = pl.BlockSpec(memory_space=pltpu.VMEM)
    hbm = pl.BlockSpec(memory_space=pltpu.HBM)
    v = pltpu.VMEM
    dma = pltpu.SemaphoreType.DMA
    qw = wide // 4
    two = 2 * rows
    scratch = [v(a.shape, a.dtype) for a in args[1:]] + [
        v((tf.shape[0], 256), BF16),
        v((2, tf.shape[0] + rows, 128), BF16),
        v((2, tf.shape[0] + rows, 128), BF16),
        v((rows, 256), BF16),
        v((rows, 256), BF16),
        v((n_ep, 4, rows, qw), BF16),
        v((n_ep, 2 * routes.shape[1], rows), F32),
        v((n_ep, exp_dev * cap, rows), BF16),
        v((n_ep, exp_dev, rows, exp_dev * cap), BF16),
        v((n_ep, exp_dev, cap, 1), F32),
        v((exp_dev, 2 * cap, wide), BF16),
        v((n_ep * exp_dev * cap, hidden), BF16),
        v((n_ep * rows, exp_dev * hidden), BF16),
        v((rows, sg.shape[1]), BF16),
        v((4, mrows, wide), BF16),
        v((2, mrows, wide), BF16),
        v((mrows, wide), BF16),
        v((mrows, wide), BF16),
        v((4, 2, two, qw), BF16),
        v((4, 2, two, qw), BF16),
        v((4, 2, two, qw), BF16),
        v((4, 2, rows, qw), BF16),
        v((4, 2, rows, qw), BF16),
        v((4, rows, qw), BF16),
        v((4, rows, qw), BF16),
        v((3, rows, qw), BF16),
        v((3, rows, qw), BF16),
        v((rows, qw), F32),
        dma((18,)), dma((120,)), dma((120,)),
    ]
    moe_out_shape = jax.ShapeDtypeStruct((rows, qw), BF16)
    mix_out_shape = jax.ShapeDtypeStruct((mrows, wide), BF16)
    return pl.pallas_call(
        functools.partial(fused_kernel, cap),
        out_shape=(mix_out_shape, moe_out_shape),
        in_specs=[pl.BlockSpec(memory_space=pltpu.SMEM)] + [hbm] * (len(args) - 1),
        out_specs=(vm, vm),
        scratch_shapes=scratch,
        compiler_params=pltpu.CompilerParams(
            collective_id=0, has_side_effects=True, vmem_limit_bytes=50 * 1024 * 1024
        ),
        name="fused",
    )(*args)


def local(
    tokens_first,
    attn_gain,
    w_query,
    key_matrix,
    value_matrix,
    head_sink_logit,
    w_output,
    tokens_second,
    ffn_gain,
    routes,
    route_weight,
    w_gate_exp,
    w_up_exp,
    w_down_exp,
    w_gate_shared,
    w_up_shared,
    w_down_shared,
):
    if lax.axis_size("ep") == 8 and lax.axis_size("tp") == 4:
        return fused(
            tokens_first, attn_gain, w_query, key_matrix, value_matrix, head_sink_logit, w_output,
            tokens_second, ffn_gain, routes, route_weight, w_gate_exp, w_up_exp, w_down_exp,
            w_gate_shared, w_up_shared, w_down_shared,
        )
    rows_first = tokens_first.shape[0]
    norm_input = rms_scale(tokens_first, attn_gain)
    offset = lax.axis_index("ep") * rows_first
    token_positions = (offset + jnp.arange(rows_first, dtype=jnp.int32)).astype(jnp.float32)
    head_count = w_query.shape[1] // HEAD_SIZE
    key_heads = key_matrix.shape[1] // HEAD_SIZE
    head_group = head_count // key_heads
    query_rows = apply_rotary(
        jnp.dot(norm_input, w_query, preferred_element_type=jnp.float32).reshape(
            rows_first, head_count, HEAD_SIZE
        ),
        token_positions,
    ).astype(jnp.bfloat16)
    keys_local = apply_rotary(
        jnp.dot(norm_input, key_matrix, preferred_element_type=jnp.float32).reshape(
            rows_first, key_heads, HEAD_SIZE
        ),
        token_positions,
    ).astype(jnp.bfloat16)
    values_local = (
        jnp.dot(norm_input, value_matrix, preferred_element_type=jnp.float32)
        .astype(jnp.bfloat16)
        .reshape(rows_first, key_heads, HEAD_SIZE)
    )
    keys_before, values_before = from_behind(
        (keys_local[rows_first - BAND_LENGTH :], values_local[rows_first - BAND_LENGTH :]),
        "ep",
        1,
    )
    keys_all = jnp.concatenate([keys_before, keys_local], axis=0)
    values_all = jnp.concatenate([values_before, values_local], axis=0)
    band = BAND_LENGTH
    bands = rows_first // band

    def windows(padded):
        return jnp.concatenate(
            [
                padded[:rows_first].reshape(bands, band, key_heads, HEAD_SIZE),
                padded[band:].reshape(bands, band, key_heads, HEAD_SIZE),
            ],
            axis=1,
        )

    sink_scores = head_sink_logit.reshape(key_heads, head_group)[None, :, :, None, None]
    scores = jnp.einsum(
        "bqhgd,bkhd->bhgqk",
        query_rows.reshape(bands, band, key_heads, head_group, HEAD_SIZE),
        windows(keys_all),
        preferred_element_type=jnp.float32,
    ) * HEAD_SIZE ** (-0.5)
    offsets = (
        band
        + jnp.arange(band, dtype=jnp.int32)[:, None]
        - jnp.arange(2 * band, dtype=jnp.int32)[None, :]
    )
    key_pos = (
        offset
        + (jnp.arange(bands, dtype=jnp.int32)[:, None] - 1) * band
        + jnp.arange(2 * band, dtype=jnp.int32)[None, :]
    )
    visible = ((offsets >= 0) & (offsets < band))[None] & (key_pos >= 0)[:, None, :]
    scores = jnp.where(visible[:, None, None], scores, -jnp.inf)
    peak = jnp.maximum(jnp.max(scores, axis=-1, keepdims=True), sink_scores)
    expo = jnp.exp(scores - peak)
    total = jnp.sum(expo, axis=-1, keepdims=True) + jnp.exp(sink_scores - peak)
    weights = (expo / total).astype(jnp.bfloat16)
    attended = (
        jnp.einsum(
            "bhgqk,bkhd->bqhgd", weights, windows(values_all), preferred_element_type=jnp.float32
        )
        .astype(jnp.bfloat16)
        .reshape(rows_first, head_count * HEAD_SIZE)
    )
    mixer_out = lax.psum_scatter(
        jnp.dot(attended, w_output, preferred_element_type=jnp.float32).astype(jnp.bfloat16),
        "tp",
        scatter_dimension=0,
        tiled=True,
    )
    rows_second = tokens_second.shape[0]
    topk = routes.shape[1]
    exp_dev = w_gate_exp.shape[0]
    n_expdev = lax.axis_size("ep")
    experts = exp_dev * n_expdev
    capacity = max(2, 2 * rows_second * topk // experts)
    slot_count = experts * capacity
    normed_second = rms_scale(tokens_second, ffn_gain)
    flat = routes.reshape(-1)
    onehot = (flat[:, None] == jnp.arange(experts, dtype=jnp.int32)[None, :]).astype(jnp.int32)
    ranks = jnp.sum((jnp.cumsum(onehot, axis=0) - onehot) * onehot, axis=1)
    slots = flat * capacity + ranks
    match = (jnp.arange(slot_count, dtype=jnp.int32)[:, None] == slots[None, :]).reshape(
        slot_count, rows_second, topk
    )
    dispatch = jnp.sum(match.astype(jnp.float32), axis=2).astype(jnp.bfloat16)
    combine = jnp.sum(match.astype(jnp.float32) * route_weight[None, :, :], axis=2)
    width = normed_second.shape[1] // lax.axis_size("tp")
    feature_slice = lax.dynamic_slice_in_dim(normed_second, lax.axis_index("tp") * width, width, 1)
    outgoing = jnp.dot(dispatch, feature_slice, preferred_element_type=jnp.float32).astype(
        jnp.bfloat16
    )
    arrived = lax.all_to_all(outgoing, "ep", split_axis=0, concat_axis=0, tiled=True)
    piece = lax.all_gather(arrived, "tp", axis=1, tiled=True)
    cols = piece.shape[1]
    part = piece.reshape(n_expdev, exp_dev, capacity, cols)
    gate_pre = jnp.einsum("sjcd,jdf->sjcf", part, w_gate_exp, preferred_element_type=jnp.float32)
    up_pre = jnp.einsum("sjcd,jdf->sjcf", part, w_up_exp, preferred_element_type=jnp.float32)
    hidden = (jax.nn.silu(gate_pre) * up_pre).astype(jnp.bfloat16)
    shared_hidden = (
        jax.nn.silu(jnp.dot(normed_second, w_gate_shared, preferred_element_type=jnp.float32))
        * jnp.dot(normed_second, w_up_shared, preferred_element_type=jnp.float32)
    ).astype(jnp.bfloat16)
    routed_term = jnp.einsum(
        "sjcf,jfd->dsjc", hidden, w_down_exp, preferred_element_type=jnp.float32
    ).reshape(lax.axis_size("tp") * (MODEL_WIDTH // lax.axis_size("tp")), slot_count)
    shared_term = lax.dot_general(
        w_down_shared, shared_hidden, (((0,), (1,)), ((), ())), preferred_element_type=jnp.float32
    )
    summed = lax.psum_scatter(
        jnp.concatenate([routed_term, shared_term], axis=1).astype(jnp.bfloat16),
        "tp",
        scatter_dimension=0,
        tiled=True,
    ).astype(jnp.float32)
    routed_part = summed[:, :slot_count].astype(jnp.bfloat16)
    returned = lax.all_to_all(routed_part, "ep", split_axis=1, concat_axis=1, tiled=True)
    weighted = lax.dot_general(
        combine,
        returned.astype(jnp.float32),
        (((0,), (1,)), ((), ())),
        precision=lax.Precision.HIGHEST,
    )
    moe_out = (weighted + summed[:, slot_count:].T).astype(jnp.bfloat16)
    return (mixer_out, moe_out)


def solution(mesh):
    in_specs = (
        P("ep", None),
        P(),
        P(None, "tp"),
        P(None, "tp"),
        P(None, "tp"),
        P("tp"),
        P("tp", None),
        P("ep", None),
        P(),
        P("ep", None),
        P("ep", None),
        P("ep", None, "tp"),
        P("ep", None, "tp"),
        P("ep", "tp", None),
        P(None, "tp"),
        P(None, "tp"),
        P("tp", None),
    )
    out_specs = (P(("ep", "tp"), None), P("ep", "tp"))
    return jax.shard_map(local, mesh=mesh, in_specs=in_specs, out_specs=out_specs, check_vma=False)
```

```python
import functools
import jax
import jax.numpy as jnp
import numpy as np
from jax import lax
from jax.experimental import pallas as pl
from jax.experimental.pallas import tpu as pltpu
from jax.sharding import PartitionSpec as P

MODEL_WIDTH = 2048
HEAD_SIZE = 64
BAND_LENGTH = 128


rope_base = 10000.0
norm_eps = 1e-06


def from_behind(value, axis, by):
    devices = lax.axis_size(axis)
    pairs = [(i, i + by) for i in range(devices) if 0 <= i + by < devices]
    return lax.ppermute(value, axis, pairs)


def rms_scale(inputs, gain):
    wide = inputs.astype(jnp.float32)
    scaled = wide * lax.rsqrt(jnp.mean(wide * wide, axis=-1, keepdims=True) + norm_eps)
    return (scaled * gain).astype(jnp.bfloat16)


def apply_rotary(heads, token_positions):
    freqs = rope_base ** (-jnp.arange(0, HEAD_SIZE, 2, dtype=jnp.float32) / HEAD_SIZE)
    angles = token_positions[:, None] * freqs[None, :]
    cosine = jnp.cos(angles)[:, None, :]
    sine = jnp.sin(angles)[:, None, :]
    first_half, second_half = jnp.split(heads, 2, axis=-1)
    return jnp.concatenate(
        [first_half * cosine - second_half * sine, second_half * cosine + first_half * sine],
        axis=-1,
    )


MESH = pl.DeviceIdType.MESH
F32 = jnp.float32
BF16 = jnp.bfloat16


def dot(a, b):
    return jnp.dot(a, b, preferred_element_type=F32)


def scoped(f):
    def call(*a):
        with jax.named_scope("_".join([f.__name__] + [str(v) for v in a if isinstance(v, int)])):
            return f(*a)

    return call


def lanes_of(shape):
    return lax.broadcasted_iota(jnp.int32, shape, len(shape) - 1)


def fused_kernel(
    cap,
    sinks, ag_h, fg_h, rt_h, rw_h, fine_h, coarse_h, tf_h, wq_h, wk_h, wv_h, wo_h, ts_h,
    wg_h, wu_h, wd_h, sg_h, su_h, sd_h,
    mix_out, moe_out,
    ag, fg, rt, rw, fine, coarse, tf, wq, wk, wv, wo, ts, wg, wu, wd, sg, su, sd,
    qs, kd, vd, halo_s, halo_r, xg, mg, oh, oht, wsl, xs, hid, tokh, shh,
    mp, mrc, ms, mry, mo_own, mo_peer, rc, s1x, rx1, s2y, ry2, s3, rz, s4, rl, keep,
    lsem, ss, rs,
):
    me, t = lax.axis_index("ep"), lax.axis_index("tp")
    z, x, y, c = me // 2, me % 2, t // 2, t % 2
    zs = (z, z + 1 - 2 * (z % 2), (z + 2) % 4, 3 - z)
    z_peer = [{"ep": zd * 2 + x, "tp": t} for zd in zs]
    x_peer = {"ep": z * 2 + 1 - x, "tp": t}
    y_peer = {"ep": me, "tp": (1 - y) * 2 + c}
    zy_peer = {"ep": zs[1] * 2 + x, "tp": (1 - y) * 2 + c}
    c_peer = {"ep": me, "tp": y * 2 + 1 - c}
    n_ep = 8
    exp_dev = wg.shape[0]
    topk = rt.shape[0]
    rows = ts.shape[0]
    blocks = tf.shape[0] // rows

    loads = {}

    def load(name, src, dst):
        k = pltpu.make_async_copy(src, dst, lsem.at[len(loads)])
        k.start()
        loads[name] = k

    def need(*names):
        for name in names:
            k = loads.pop(name, None)
            if k is not None:
                done.append(name)
                k.wait()

    done = []
    pairs = [
        ("ts", ts_h, ts), ("fg", fg_h, fg), ("rt", rt_h, rt), ("rw", rw_h, rw), ("ag", ag_h, ag),
        ("tf", tf_h, tf), ("fine", fine_h, fine), ("coarse", coarse_h, coarse), ("wq", wq_h, wq),
        ("wk", wk_h, wk), ("wv", wv_h, wv), ("wo", wo_h, wo), ("sg", sg_h, sg), ("su", su_h, su),
        ("wg", wg_h, wg), ("wu", wu_h, wu), ("wd", wd_h, wd), ("sd", sd_h, sd),
    ]
    for name, a, b in pairs:
        load(name, a, b)

    barrier = pltpu.get_barrier_semaphore()
    for e in range(1, n_ep):
        pl.semaphore_signal(
            barrier, inc=1, device_id={"ep": (me + e) % n_ep, "tp": t}, device_id_type=MESH
        )
    for peer in (y_peer, c_peer, zy_peer):
        pl.semaphore_signal(barrier, inc=1, device_id=peer, device_id_type=MESH)

    ids = {}
    started = []

    together = {"m": mg.at[0 : n_ep - 1], "rc": rc, "rx1": rx1}
    for way in "xyzc":
        together[way] = xg.at[0 : n_ep - 1]
    groups = {}

    def copy(name, src, dst, peer):
        i = ids.setdefault(name, len(ids))
        kind = name[0] if isinstance(name, tuple) else name
        kind = "x" if kind in "xyzc" else kind
        key = kind if kind in together else name
        j = groups.setdefault(key, len(groups))
        return pltpu.make_async_remote_copy(
            src_ref=src, dst_ref=dst, send_sem=ss.at[j], recv_sem=rs.at[i],
            device_id=peer, device_id_type=MESH,
        )

    def send(name, src, dst, peer):
        k = copy(name, src, dst, peer)
        k.start()
        kind = name[0] if isinstance(name, tuple) else name
        if kind not in together:
            started.append(k)

    def got(name, dst):
        copy(name, dst, dst, c_peer).wait_recv()

    def normed(wide, gain):
        return (
            wide * lax.rsqrt(jnp.mean(wide * wide, axis=-1, keepdims=True) + norm_eps) * gain
        ).astype(BF16)

    turn = (0, 3, 1, 2)

    def R(d, s):
        return turn[d] * 2 + s

    own = R(0, 1)
    quarter = xg.shape[3]

    def q_of(k, cc):
        return (y if k else 1 - y) * 2 + cc

    parts = 2
    sub = rows // parts

    def piece(at, q, p):
        return xg.at[at, q, p * sub : (p + 1) * sub, :]

    def block_send(link, k, peer, at, p):
        q = q_of(k, c)
        send((link, at, k, p), piece(own, q, p), piece(at, q, p), peer)

    @scoped
    def norm_second(p):
        part = slice(p * sub, (p + 1) * sub)
        xn = normed(ts[part].astype(F32), fg[...])
        for q in range(4):
            xg[own, q, part] = xn[:, q * quarter : (q + 1) * quarter]

    @scoped
    def barrier_wait():
        pl.semaphore_wait(barrier, n_ep + 2)

    need("ts", "fg", "rt", "rw")
    mg[own] = jnp.concatenate([rt[...].astype(F32), rw[...]], axis=0)
    for p in range(parts):
        norm_second(p)
        if p == 0:
            barrier_wait()
            for s in (0, 1):
                for d in range(4):
                    if R(d, s) != own:
                        peer = {"ep": zs[d] * 2 + (x if s else 1 - x), "tp": t}
                        send(("m", R(d, s)), mg.at[own], mg.at[R(d, s)], peer)
        block_send("z", 1, z_peer[2], R(2, 1), p)
        block_send("x", 1, x_peer, R(0, 0), p)

    def send_three():
        for p in range(parts):
            block_send("z", 1, z_peer[3], R(3, 1), p)

    def send_one():
        for p in range(parts):
            block_send("z", 1, z_peer[1], R(1, 1), p)
            block_send("z", 0, z_peer[1], R(1, 1), p)

    def arrive(link, d, s, k, p, *onward):
        at, q = R(d, s), q_of(k, c)
        here = piece(at, q, p)
        with jax.named_scope("%s_d%d_s%d_k%d_p%d" % (link, d, s, k, p)):
            got((link, at, k, p), here)
        for way in onward:
            if way == "x":
                send(("x", R(d, 0), k, p), here, piece(R(d, 0), q, p), x_peer)
            else:
                send(("y", at, 0, p), here, here, y_peer)
        send(("c", at, k, p), here, here, c_peer)

    @scoped
    def from_core(at):
        for p in range(parts):
            for k in (1, 0):
                got(("c", at, k, p), piece(at, q_of(k, 1 - c), p))

    lane = lanes_of((rows, 128))
    low = lane % 64 < 32
    left = lane < 64

    @scoped
    def qkv(b):
        part = slice(b * rows, (b + 1) * rows)
        nb = normed(tf[part].astype(F32), ag[...])
        base = pl.ds(me * blocks + b, 1)
        cb, sb = coarse[0, base, :], coarse[1, base, :]
        cosine = fine[0] * cb - fine[1] * sb
        sine = fine[1] * cb + fine[0] * sb
        sine = jnp.where(low, -sine, sine)

        def rot(v):
            swap = jnp.where(low, pltpu.roll(v, 96, 1), pltpu.roll(v, 32, 1))
            return v * cosine + swap * sine

        need("wk")
        kk = rot(dot(nb, wk[...]))
        need("wv")
        vv = dot(nb, wv[...])
        store_kv(kk.astype(BF16).astype(F32), vv.astype(BF16).astype(F32), (b + 1) * rows)
        if b == blocks - 1:
            halo_s[:, 0:128] = kk.astype(BF16)
            halo_s[:, 128:256] = vv.astype(BF16)
        need("wq")
        for g in range(2):
            qq = rot(dot(nb, wq[:, g * 128 : (g + 1) * 128])) * HEAD_SIZE ** (-0.5)
            qs[part, g * 128 : (g + 1) * 128] = qq.astype(BF16)

    def store_kv(kk, vv, at):
        for ref, val in ((kd, kk), (vd, vv)):
            other = pltpu.roll(val, 64, 1)
            ref[0, at : at + rows, :] = jnp.where(left, val, other).astype(BF16)
            ref[1, at : at + rows, :] = jnp.where(left, other, val).astype(BF16)

    i2 = lax.broadcasted_iota(jnp.int32, (2 * rows, 2 * rows), 0)
    band = lanes_of((2 * rows, 2 * rows)) - i2 % rows
    top = lax.broadcasted_iota(jnp.int32, (2 * rows, 1), 0) < rows

    @scoped
    def attend(b):
        part = slice(b * rows, (b + 1) * rows)
        outs = []
        visible = (band > 0) & (band <= rows)
        if b == 0:
            visible = visible & ((lanes_of((2 * rows, 2 * rows)) >= rows) | (me > 0))
        for g in range(2):
            q2 = qs[part, g * 128 : (g + 1) * 128]
            zero = jnp.zeros_like(q2)
            qq = jnp.concatenate([jnp.where(left, q2, zero), jnp.where(left, zero, q2)], axis=0)
            score = lax.dot_general(
                qq, kd[g, b * rows : (b + 2) * rows, :], (((1,), (1,)), ((), ())),
                preferred_element_type=F32,
            )
            score = jnp.where(visible, score, -jnp.inf)
            sink = jnp.where(top, sinks[2 * g], sinks[2 * g + 1])
            peak = jnp.maximum(jnp.max(score, axis=-1, keepdims=True), sink)
            expo = jnp.exp(score - peak)
            total = jnp.sum(expo, axis=-1, keepdims=True) + jnp.exp(sink - peak)
            weights = (expo * (1.0 / total)).astype(BF16)
            o = dot(weights, vd[g, b * rows : (b + 2) * rows, :])
            outs.append(jnp.where(left, o[:rows], o[rows:]).astype(BF16))
        att = jnp.concatenate(outs, axis=1)
        need("wo")
        for n in range(4):
            mp[b, :, n * 512 : (n + 1) * 512] = dot(att, wo[:, n * 512 : (n + 1) * 512]).astype(BF16)

    @scoped
    def onehots():
        for s in (0, 1):
            for d in range(4):
                if R(d, s) != own:
                    got(("m", R(d, s)), mg.at[R(d, s)])
        before = (
            lax.broadcasted_iota(jnp.int32, (rows, rows), 0)
            < lax.broadcasted_iota(jnp.int32, (rows, rows), 1)
        ).astype(F32).astype(BF16)
        hits, vals = [], []
        for r in range(n_ep):
            for e in range(exp_dev):
                named = mg[r, 0:topk, :] == (me * exp_dev + e).astype(F32)
                hits.append(jnp.sum(named.astype(F32), axis=0, keepdims=True))
                vals.append(
                    jnp.sum(jnp.where(named, mg[r, topk : 2 * topk, :], 0.0), axis=0, keepdims=True)
                )
        ranks = dot(jnp.concatenate(hits, axis=0).astype(BF16), before)
        slot = lax.broadcasted_iota(jnp.int32, (cap, rows), 0).astype(F32)
        for r in range(n_ep):
            both = []
            for e in range(exp_dev):
                i = r * exp_dev + e
                at = (slot == ranks[i : i + 1, :]) & (hits[i] > 0.0)
                both.append(at.astype(F32))
                wsl[r, e] = jnp.sum(jnp.where(at, vals[i], 0.0), axis=1, keepdims=True)
            full = jnp.concatenate(both, axis=0)
            oh[r] = full.astype(BF16)
            turned = full.T
            for e in range(exp_dev):
                oht[r, e] = jnp.where(lanes_of(turned.shape) // cap == e, turned, 0.0).astype(BF16)

    @scoped
    def shared_hidden():
        need("sg", "su")
        g = jnp.zeros((rows, sg.shape[1]), F32)
        u = jnp.zeros((rows, sg.shape[1]), F32)
        for q in range(4):
            part = slice(q * quarter, (q + 1) * quarter)
            g = g + dot(xg[own, q], sg[part, :])
            u = u + dot(xg[own, q], su[part, :])
        shh[...] = (g / (1.0 + jnp.exp(-g)) * u).astype(BF16)

    def pair(d):
        return (R(d, 0), R(d, 1))

    @scoped
    def dispatch(d):
        for i, r in enumerate(pair(d)):
            for q in range(4):
                v = dot(oh[r], xg[r, q]).astype(BF16)
                for e in range(exp_dev):
                    xs[e, i * cap : (i + 1) * cap, q * quarter : (q + 1) * quarter] = v[
                        e * cap : (e + 1) * cap
                    ]

    @scoped
    def gate_up(d, e):
        need("wg", "wu")
        wcol = jnp.concatenate([wsl[r, e] for r in pair(d)], axis=0)
        for n in range(hid.shape[1] // 256):
            cs = slice(n * 256, (n + 1) * 256)
            g = dot(xs[e], wg[e, :, cs])
            u = dot(xs[e], wu[e, :, cs])
            hh = (g / (1.0 + jnp.exp(-g)) * u * wcol).astype(BF16)
            for i, r in enumerate(pair(d)):
                hid[r * rows + e * cap : r * rows + (e + 1) * cap, cs] = hh[i * cap : (i + 1) * cap]

    @scoped
    def to_tokens(d):
        width = hid.shape[1]
        for r in pair(d):
            for e in range(exp_dev):
                tokh[r * rows : (r + 1) * rows, e * width : (e + 1) * width] = dot(
                    oht[r, e], hid[r * rows : (r + 1) * rows, :]
                ).astype(BF16)

    ysel = (1 - y, y)

    @scoped
    def down(d, yr, peer):
        need("wd", "sd")
        i = turn[d]
        cc = 1 - c if peer else c
        out = mo_peer if peer else mo_own
        width = hid.shape[1]
        part = slice(i * 256, (i + 1) * 256)
        for n in range(2):
            base = pl.multiple_of((ysel[yr] * 2 + cc) * 512 + n * 256, 256)
            cs = pl.ds(base, 256)
            v = dot(tokh[part, 0:width], wd[0, :, cs]) + dot(tokh[part, width : 2 * width], wd[1, :, cs])
            if d == 0:
                v = jnp.concatenate([v[:rows], v[rows:] + dot(shh[...], sd[:, cs])], axis=0)
            out[i, yr, :, n * 256 : (n + 1) * 256] = v.astype(BF16)
        if peer:
            send(("rc", i, yr), mo_peer.at[i, yr], rc.at[i, yr], c_peer)

    def span(h):
        return pl.ds(0, 512) if h is None else pl.ds(h * 256, 256)

    def both(i, yr, part, h=None):
        at = span(h)
        return mo_own[i, yr, part, at].astype(F32) + rc[i, yr, part, at].astype(F32)

    far, near = slice(0, 128), slice(128, 256)

    @scoped
    def stage1(d, yr, h=None):
        i, at = turn[d], span(h)
        if not h:
            got(("rc", i, yr), rc.at[i, yr])
        s1x[i, yr, :, at] = both(i, yr, far, h).astype(BF16)
        send(("rx1", i, yr, h), s1x.at[i, yr, :, at], rx1.at[i, yr, :, at], x_peer)

    @scoped
    def stage2(d):
        i = turn[d]
        got(("rx1", i, 0, None), rx1.at[i, 0])
        s2y[i] = (both(i, 0, near) + rx1[i, 0].astype(F32)).astype(BF16)
        send(("ry2", i), s2y.at[i], ry2.at[i], y_peer)

    @scoped
    def last(yr, h):
        i, at = turn[1], span(h)
        got(("rx1", i, yr, h), rx1.at[i, yr, :, at])
        s4[yr, :, at] = (both(i, yr, near, h) + rx1[i, yr, :, at].astype(F32)).astype(BF16)
        send(("rl", yr, h), s4.at[yr, :, at], rl.at[yr, :, at], z_peer[1] if yr else zy_peer)

    @scoped
    def stage3(d):
        i = turn[d]
        got(("rx1", i, 1, None), rx1.at[i, 1])
        v = both(i, 1, near) + rx1[i, 1].astype(F32)
        got(("ry2", i), ry2.at[i])
        v = v + ry2[i].astype(F32)
        if d:
            s3[d - 2] = v.astype(BF16)
            send(("rz", d), s3.at[d - 2], rz.at[d - 2], z_peer[d])
        else:
            keep[...] = v

    @scoped
    def final():
        v = keep[...]
        for d in (2, 3):
            got(("rz", d), rz.at[d - 2])
            v = v + rz[d - 2].astype(F32)
        for h in range(2):
            at = span(h)
            u = v[:, h * 256 : (h + 1) * 256]
            for yr in range(2):
                got(("rl", yr, h), rl.at[yr, :, at])
                u = u + rl[yr, :, at].astype(F32)
            moe_out[:, at] = u.astype(BF16)

    @scoped
    def mixer_sum():
        got(("mrc", 0), mrc.at[0])
        ms[...] = (mp[ysel[0] * 2 + c].astype(F32) + mrc[0].astype(F32)).astype(BF16)

    def mixer_rows(i):
        return pl.ds(i * (rows // 4), rows // 4)

    def mixer_send(i):
        send(("mry", i), ms.at[mixer_rows(i)], mry.at[mixer_rows(i)], y_peer)

    @scoped
    def mixer_final():
        got(("mrc", 1), mrc.at[1])
        for i in range(4):
            got(("mry", i), mry.at[mixer_rows(i)])
        mix_out[...] = (
            mp[ysel[1] * 2 + c].astype(F32) + mrc[1].astype(F32) + mry[...].astype(F32)
        ).astype(BF16)

    @scoped
    def halo_in():
        @pl.when(me == 0)
        def _():
            halo_r[...] = jnp.zeros_like(halo_r)

        @pl.when(me > 0)
        def _():
            got("halo", halo_r)

        store_kv(halo_r[:, 0:128].astype(F32), halo_r[:, 128:256].astype(F32), 0)

    need("ag", "tf", "fine", "coarse")
    qkv(3)

    @pl.when(me < n_ep - 1)
    def _():
        copy("halo", halo_s, halo_r, {"ep": (me + 1) % n_ep, "tp": t}).start()

    def cores(d):
        for r in pair(d):
            if r != own:
                from_core(r)

    qkv(0)
    qkv(1)
    arrive("x", 0, 0, 1, 0, "y")
    arrive("x", 0, 0, 1, 1, "y")
    qkv(2)
    send_three()
    attend(1)
    arrive("z", 2, 1, 1, 0, "y", "x")
    onehots()
    attend(2)
    arrive("y", 0, 0, 0, 0)
    arrive("z", 2, 1, 1, 1, "y", "x")
    shared_hidden()
    send_one()
    attend(3)
    arrive("y", 0, 0, 0, 1)
    arrive("y", 2, 1, 0, 0)
    halo_in()
    attend(0)
    for k in (0, 1):
        send(("mrc", k), mp.at[ysel[k] * 2 + 1 - c], mrc.at[k], c_peer)
    arrive("x", 2, 0, 1, 0, "y")
    cores(0)
    dispatch(0)
    gate_up(0, 0)
    arrive("y", 2, 1, 0, 1)
    arrive("z", 3, 1, 1, 0, "x", "y")
    gate_up(0, 1)
    to_tokens(0)
    arrive("x", 2, 0, 1, 1, "y")
    down(0, 0, True)
    arrive("y", 2, 0, 0, 0)
    arrive("z", 1, 1, 1, 0, "x")
    down(0, 1, True)
    arrive("z", 3, 1, 1, 1, "x", "y")
    down(0, 0, False)
    arrive("z", 1, 1, 0, 0, "x")
    stage1(0, 0)
    down(0, 1, False)
    arrive("x", 3, 0, 1, 0, "y")
    arrive("y", 2, 0, 0, 1)
    arrive("y", 3, 1, 0, 0)
    arrive("z", 1, 1, 1, 1, "x")
    cores(2)
    dispatch(2)
    arrive("z", 1, 1, 0, 1, "x")
    stage1(0, 1)
    gate_up(2, 0)
    gate_up(2, 1)
    to_tokens(2)
    arrive("x", 3, 0, 1, 1, "y")
    mixer_sum()
    mixer_send(0)
    mixer_send(1)
    down(2, 0, True)
    down(2, 1, True)
    arrive("y", 3, 1, 0, 1)
    arrive("y", 3, 0, 0, 0)
    down(2, 0, False)
    stage1(2, 0)
    down(2, 1, False)
    stage1(2, 1)
    arrive("y", 3, 0, 0, 1)
    stage2(0)
    mixer_send(2)
    cores(3)
    dispatch(3)
    arrive("x", 1, 0, 1, 0)
    arrive("x", 1, 0, 0, 0)
    gate_up(3, 0)
    arrive("x", 1, 0, 1, 1)
    gate_up(3, 1)
    arrive("x", 1, 0, 0, 1)
    to_tokens(3)
    down(3, 0, True)
    down(3, 1, True)
    down(3, 0, False)
    stage1(3, 0)
    down(3, 1, False)
    stage1(3, 1)
    cores(1)
    dispatch(1)
    stage2(2)
    gate_up(1, 0)
    gate_up(1, 1)
    to_tokens(1)
    down(1, 0, True)
    down(1, 1, True)
    stage2(3)
    mixer_send(3)
    down(1, 0, False)
    stage1(1, 0, 0)
    stage1(1, 0, 1)
    stage3(2)
    down(1, 1, False)
    stage1(1, 1, 0)
    stage1(1, 1, 1)
    stage3(3)
    last(0, 0)
    last(0, 1)
    last(1, 0)
    last(1, 1)
    stage3(0)
    mixer_final()
    final()

    @pl.when(me < n_ep - 1)
    def _():
        copy("halo", halo_s, halo_r, {"ep": (me + 1) % n_ep, "tp": t}).wait_send()

    @scoped
    def all_sent():
        for k in started:
            k.wait_send()
        for kind in ("x", "m", "rc", "rx1"):
            whole, sem = together[kind], ss.at[groups[kind]]
            pltpu.make_async_remote_copy(
                src_ref=whole, dst_ref=whole, send_sem=sem, recv_sem=sem,
                device_id=c_peer, device_id_type=MESH,
            ).wait_send()

    all_sent()
    assert not loads and (len(ids), len(groups)) == (rs.shape[0], ss.shape[0]), (len(ids), len(groups))


def rope_tables(tokens, rows):
    freqs = rope_base ** (-np.arange(0, HEAD_SIZE, 2) / HEAD_SIZE)
    freqs = np.tile(freqs, 128 // len(freqs))
    fine = np.arange(rows)[:, None] * freqs[None, :]
    coarse = np.arange(0, tokens, rows)[:, None] * freqs[None, :]
    return [
        jnp.asarray(np.stack([np.cos(a), np.sin(a)]), dtype=jnp.float32) for a in (fine, coarse)
    ]


def fused(tf, ag, wq, wk, wv, sink, wo, ts, fg, routes, rweight, wg, wu, wd, sg, su, sd):
    n_ep = lax.axis_size("ep")
    rows, wide = ts.shape
    exp_dev, _, hidden = wg.shape
    cap = max(2, 2 * rows * routes.shape[1] // (exp_dev * n_ep))
    mrows = tf.shape[0] // 4
    fine, coarse = rope_tables(tf.shape[0] * n_ep, rows)
    args = (
        sink, ag.reshape(1, -1), fg.reshape(1, -1), routes.T, rweight.T, fine, coarse,
        tf, wq, wk, wv, wo, ts, wg, wu, wd, sg, su, sd,
    )
    args = tuple(pltpu.with_memory_space_constraint(a, pltpu.HBM) for a in args)
    vm = pl.BlockSpec(memory_space=pltpu.VMEM)
    hbm = pl.BlockSpec(memory_space=pltpu.HBM)
    v = pltpu.VMEM
    dma = pltpu.SemaphoreType.DMA
    qw = wide // 4
    two = 2 * rows
    scratch = [v(a.shape, a.dtype) for a in args[1:]] + [
        v((tf.shape[0], 256), BF16),
        v((2, tf.shape[0] + rows, 128), BF16),
        v((2, tf.shape[0] + rows, 128), BF16),
        v((rows, 256), BF16),
        v((rows, 256), BF16),
        v((n_ep, 4, rows, qw), BF16),
        v((n_ep, 2 * routes.shape[1], rows), F32),
        v((n_ep, exp_dev * cap, rows), BF16),
        v((n_ep, exp_dev, rows, exp_dev * cap), BF16),
        v((n_ep, exp_dev, cap, 1), F32),
        v((exp_dev, 2 * cap, wide), BF16),
        v((n_ep * exp_dev * cap, hidden), BF16),
        v((n_ep * rows, exp_dev * hidden), BF16),
        v((rows, sg.shape[1]), BF16),
        v((4, mrows, wide), BF16),
        v((2, mrows, wide), BF16),
        v((mrows, wide), BF16),
        v((mrows, wide), BF16),
        v((4, 2, two, qw), BF16),
        v((4, 2, two, qw), BF16),
        v((4, 2, two, qw), BF16),
        v((4, 2, rows, qw), BF16),
        v((4, 2, rows, qw), BF16),
        v((4, rows, qw), BF16),
        v((4, rows, qw), BF16),
        v((2, rows, qw), BF16),
        v((2, rows, qw), BF16),
        v((2, rows, qw), BF16),
        v((2, rows, qw), BF16),
        v((rows, qw), F32),
        dma((18,)), dma((20,)), dma((97,)),
    ]
    moe_out_shape = jax.ShapeDtypeStruct((rows, qw), BF16)
    mix_out_shape = jax.ShapeDtypeStruct((mrows, wide), BF16)
    return pl.pallas_call(
        functools.partial(fused_kernel, cap),
        out_shape=(mix_out_shape, moe_out_shape),
        in_specs=[pl.BlockSpec(memory_space=pltpu.SMEM)] + [hbm] * (len(args) - 1),
        out_specs=(vm, vm),
        scratch_shapes=scratch,
        compiler_params=pltpu.CompilerParams(
            collective_id=0, has_side_effects=True, vmem_limit_bytes=50 * 1024 * 1024
        ),
        name="fused",
    )(*args)


def local(
    tokens_first,
    attn_gain,
    w_query,
    key_matrix,
    value_matrix,
    head_sink_logit,
    w_output,
    tokens_second,
    ffn_gain,
    routes,
    route_weight,
    w_gate_exp,
    w_up_exp,
    w_down_exp,
    w_gate_shared,
    w_up_shared,
    w_down_shared,
):
    if lax.axis_size("ep") == 8 and lax.axis_size("tp") == 4:
        return fused(
            tokens_first, attn_gain, w_query, key_matrix, value_matrix, head_sink_logit, w_output,
            tokens_second, ffn_gain, routes, route_weight, w_gate_exp, w_up_exp, w_down_exp,
            w_gate_shared, w_up_shared, w_down_shared,
        )
    rows_first = tokens_first.shape[0]
    norm_input = rms_scale(tokens_first, attn_gain)
    offset = lax.axis_index("ep") * rows_first
    token_positions = (offset + jnp.arange(rows_first, dtype=jnp.int32)).astype(jnp.float32)
    head_count = w_query.shape[1] // HEAD_SIZE
    key_heads = key_matrix.shape[1] // HEAD_SIZE
    head_group = head_count // key_heads
    query_rows = apply_rotary(
        jnp.dot(norm_input, w_query, preferred_element_type=jnp.float32).reshape(
            rows_first, head_count, HEAD_SIZE
        ),
        token_positions,
    ).astype(jnp.bfloat16)
    keys_local = apply_rotary(
        jnp.dot(norm_input, key_matrix, preferred_element_type=jnp.float32).reshape(
            rows_first, key_heads, HEAD_SIZE
        ),
        token_positions,
    ).astype(jnp.bfloat16)
    values_local = (
        jnp.dot(norm_input, value_matrix, preferred_element_type=jnp.float32)
        .astype(jnp.bfloat16)
        .reshape(rows_first, key_heads, HEAD_SIZE)
    )
    keys_before, values_before = from_behind(
        (keys_local[rows_first - BAND_LENGTH :], values_local[rows_first - BAND_LENGTH :]),
        "ep",
        1,
    )
    keys_all = jnp.concatenate([keys_before, keys_local], axis=0)
    values_all = jnp.concatenate([values_before, values_local], axis=0)
    band = BAND_LENGTH
    bands = rows_first // band

    def windows(padded):
        return jnp.concatenate(
            [
                padded[:rows_first].reshape(bands, band, key_heads, HEAD_SIZE),
                padded[band:].reshape(bands, band, key_heads, HEAD_SIZE),
            ],
            axis=1,
        )

    sink_scores = head_sink_logit.reshape(key_heads, head_group)[None, :, :, None, None]
    scores = jnp.einsum(
        "bqhgd,bkhd->bhgqk",
        query_rows.reshape(bands, band, key_heads, head_group, HEAD_SIZE),
        windows(keys_all),
        preferred_element_type=jnp.float32,
    ) * HEAD_SIZE ** (-0.5)
    offsets = (
        band
        + jnp.arange(band, dtype=jnp.int32)[:, None]
        - jnp.arange(2 * band, dtype=jnp.int32)[None, :]
    )
    key_pos = (
        offset
        + (jnp.arange(bands, dtype=jnp.int32)[:, None] - 1) * band
        + jnp.arange(2 * band, dtype=jnp.int32)[None, :]
    )
    visible = ((offsets >= 0) & (offsets < band))[None] & (key_pos >= 0)[:, None, :]
    scores = jnp.where(visible[:, None, None], scores, -jnp.inf)
    peak = jnp.maximum(jnp.max(scores, axis=-1, keepdims=True), sink_scores)
    expo = jnp.exp(scores - peak)
    total = jnp.sum(expo, axis=-1, keepdims=True) + jnp.exp(sink_scores - peak)
    weights = (expo / total).astype(jnp.bfloat16)
    attended = (
        jnp.einsum(
            "bhgqk,bkhd->bqhgd", weights, windows(values_all), preferred_element_type=jnp.float32
        )
        .astype(jnp.bfloat16)
        .reshape(rows_first, head_count * HEAD_SIZE)
    )
    mixer_out = lax.psum_scatter(
        jnp.dot(attended, w_output, preferred_element_type=jnp.float32).astype(jnp.bfloat16),
        "tp",
        scatter_dimension=0,
        tiled=True,
    )
    rows_second = tokens_second.shape[0]
    topk = routes.shape[1]
    exp_dev = w_gate_exp.shape[0]
    n_expdev = lax.axis_size("ep")
    experts = exp_dev * n_expdev
    capacity = max(2, 2 * rows_second * topk // experts)
    slot_count = experts * capacity
    normed_second = rms_scale(tokens_second, ffn_gain)
    flat = routes.reshape(-1)
    onehot = (flat[:, None] == jnp.arange(experts, dtype=jnp.int32)[None, :]).astype(jnp.int32)
    ranks = jnp.sum((jnp.cumsum(onehot, axis=0) - onehot) * onehot, axis=1)
    slots = flat * capacity + ranks
    match = (jnp.arange(slot_count, dtype=jnp.int32)[:, None] == slots[None, :]).reshape(
        slot_count, rows_second, topk
    )
    dispatch = jnp.sum(match.astype(jnp.float32), axis=2).astype(jnp.bfloat16)
    combine = jnp.sum(match.astype(jnp.float32) * route_weight[None, :, :], axis=2)
    width = normed_second.shape[1] // lax.axis_size("tp")
    feature_slice = lax.dynamic_slice_in_dim(normed_second, lax.axis_index("tp") * width, width, 1)
    outgoing = jnp.dot(dispatch, feature_slice, preferred_element_type=jnp.float32).astype(
        jnp.bfloat16
    )
    arrived = lax.all_to_all(outgoing, "ep", split_axis=0, concat_axis=0, tiled=True)
    piece = lax.all_gather(arrived, "tp", axis=1, tiled=True)
    cols = piece.shape[1]
    part = piece.reshape(n_expdev, exp_dev, capacity, cols)
    gate_pre = jnp.einsum("sjcd,jdf->sjcf", part, w_gate_exp, preferred_element_type=jnp.float32)
    up_pre = jnp.einsum("sjcd,jdf->sjcf", part, w_up_exp, preferred_element_type=jnp.float32)
    hidden = (jax.nn.silu(gate_pre) * up_pre).astype(jnp.bfloat16)
    shared_hidden = (
        jax.nn.silu(jnp.dot(normed_second, w_gate_shared, preferred_element_type=jnp.float32))
        * jnp.dot(normed_second, w_up_shared, preferred_element_type=jnp.float32)
    ).astype(jnp.bfloat16)
    routed_term = jnp.einsum(
        "sjcf,jfd->dsjc", hidden, w_down_exp, preferred_element_type=jnp.float32
    ).reshape(lax.axis_size("tp") * (MODEL_WIDTH // lax.axis_size("tp")), slot_count)
    shared_term = lax.dot_general(
        w_down_shared, shared_hidden, (((0,), (1,)), ((), ())), preferred_element_type=jnp.float32
    )
    summed = lax.psum_scatter(
        jnp.concatenate([routed_term, shared_term], axis=1).astype(jnp.bfloat16),
        "tp",
        scatter_dimension=0,
        tiled=True,
    ).astype(jnp.float32)
    routed_part = summed[:, :slot_count].astype(jnp.bfloat16)
    returned = lax.all_to_all(routed_part, "ep", split_axis=1, concat_axis=1, tiled=True)
    weighted = lax.dot_general(
        combine,
        returned.astype(jnp.float32),
        (((0,), (1,)), ((), ())),
        precision=lax.Precision.HIGHEST,
    )
    moe_out = (weighted + summed[:, slot_count:].T).astype(jnp.bfloat16)
    return (mixer_out, moe_out)


def solution(mesh):
    in_specs = (
        P("ep", None),
        P(),
        P(None, "tp"),
        P(None, "tp"),
        P(None, "tp"),
        P("tp"),
        P("tp", None),
        P("ep", None),
        P(),
        P("ep", None),
        P("ep", None),
        P("ep", None, "tp"),
        P("ep", None, "tp"),
        P("ep", "tp", None),
        P(None, "tp"),
        P(None, "tp"),
        P("tp", None),
    )
    out_specs = (P(("ep", "tp"), None), P("ep", "tp"))
    return jax.shard_map(local, mesh=mesh, in_specs=in_specs, out_specs=out_specs, check_vma=False)
```
